256 devices in a mesh: ep: 16 (over y, x), tp: 16 (over z, core).
Axes of the slice: x: 4, y: 4, z: 8, core: 2. Of those that a mesh axis runs over, the one named last changes fastest.
Arguments:
- queries: bfloat16 [12288, 2048], P('ep', 'tp'), may hold values from -6 to 6
- keys: bfloat16 [12288, 512], P('ep'), may hold values from -6 to 6
- values: bfloat16 [12288, 512], P('ep'), may hold values from -6 to 6
- query_gain: float32 [128], replicated, may hold values from 1 to 4.5
- key_gain: float32 [128], replicated, may hold values from 1 to 4.5
- out_weight: bfloat16 [2048, 2048], P('tp'), may hold values from -0.75 to 0.75
- tokens_b: bfloat16 [12288, 2048], P('ep'), may hold values from -6 to 6
- norm_gain: float32 [2048], replicated, may hold values from 0.1 to 1.9
- routes: int32 [12288, 2], P('ep'), may hold values from 0 to 15, all different within a row; in each aligned block of 48 rows (0 to 47, 48 to 95, ...) at most 8 rows name the same one
- route_weight: float32 [12288, 2], P('ep'), may hold values from 0.2 to 1
- gate_weight: bfloat16 [16, 2048, 4096], P('ep', None, 'tp'), may hold values from -0.125 to 0.125
- up_weight: bfloat16 [16, 2048, 4096], P('ep', None, 'tp'), may hold values from -0.125 to 0.125
- down_weight: bfloat16 [16, 4096, 2048], P('ep', 'tp'), may hold values from -0.09375 to 0.09375
Outputs:
- mixed_out: bfloat16 [12288, 2048], P(('ep', 'tp'))
- expert_out: bfloat16 [12288, 2048], P(('ep', 'tp'))
The draws below stay inside these ranges and needn't reach their ends.
Inputs may be any that keep to these rules, and one draw needn't show every extreme that they name: `routes`: A row names 2 different experts. In each aligned block of 48 rows no expert is named more than 8 times, a bound that some block reaches.
All inputs are finite; a program needn't handle non-finite values.
Results may differ from the reference program's by a relative error of at most 0.019.
Values may be sent and summed in bfloat16 or wider, within the bound.
A program may use at most 128 MiB of HBM per device.

```python
import math
import jax
import jax.numpy as jnp
import numpy as np
from jax import lax

D = 2048
HD = 128
HQ = 16
KVH = 4
GROUP = 4
FF = 4096
EXPERTS = 16
TOPK = 2
GRID_W = 64
TOK_DEV = 48
CAP = 8
LEN = 12288
TOKB = 12288
N_TP = 16


def draw_queries(key, part):
    drawn = jax.random.normal(jax.random.fold_in(key, 11), (LEN, HQ, HD), jnp.float32)
    return jnp.clip(drawn, -6.0, 6.0).reshape(LEN, HQ * HD).astype(jnp.bfloat16)


def draw_keys(key, part):
    drawn = jax.random.normal(jax.random.fold_in(key, 12), (LEN, KVH, HD), jnp.float32)
    return jnp.clip(drawn, -6.0, 6.0).reshape(LEN, KVH * HD).astype(jnp.bfloat16)


def draw_query_gain(key, part):
    uniform_g = jax.random.uniform(jax.random.fold_in(key, 13), (HD,), jnp.float32, 1.0, 2.0)
    return uniform_g


def draw_key_gain(key, part):
    uniform_g = jax.random.uniform(jax.random.fold_in(key, 14), (HD,), jnp.float32, 1.0, 2.0)
    return uniform_g


def block_scale(key, dims, pieces, smallest, top_value):
    level, own = 1.0, jax.random.fold_in(key, 6)
    for position, shards_of in pieces:
        steps = jnp.exp(jax.random.uniform(jax.random.fold_in(own, position), (shards_of,), jnp.float32, smallest / len(pieces), top_value / len(pieces)))
        level = level * jnp.repeat(steps, dims[position] // shards_of).reshape([-1 if axis == position else 1 for axis in range(len(dims))])
    return level


def deal_out(rng, own, number, rows, count, top, most, lean):
    sequence = jax.random.permutation(rng, count)
    heavy_load, common = load_shares(count, rows * top, most, lean, True), load_shares(count, rows * top, most, lean, False)
    places = jnp.arange(count)

    def named(sizes, rotation):
        used = int((sizes > 0).sum())
        fixed = max(1, used // 4)
        moved = fixed + (places - fixed + rotation * (used - fixed)) % max(1, count - fixed)
        return jnp.zeros((count,), jnp.int32).at[sequence[jnp.where(places < fixed, places, moved)]].set(jnp.asarray(sizes, jnp.int32))

    sizes = jnp.where(number % 4 == 0, named(heavy_load, number // 4), named(common, number - number // 4 - 1))
    mixed = jax.random.permutation(jax.random.fold_in(own, 3), count)
    donor, sink = mixed[0:count // 2 * 2:2], mixed[1:count // 2 * 2:2]
    room = jnp.minimum(sizes[donor] - 1, most - sizes[sink]) // 2
    room = jnp.where((donor == sequence[0]) | (sink == sequence[0]) | (sizes[sink] == 0), 0, jnp.maximum(room, 0))
    moved = jax.random.randint(jax.random.fold_in(own, 4), (count // 2,), 0, 1 << 20) % (room + 1)
    sizes = sizes.at[donor].add(-moved).at[sink].add(moved)
    labels = jnp.searchsorted(jnp.cumsum(sizes), jnp.arange(rows * top), side="right").astype(jnp.int32)
    table = labels.reshape(top, rows).T
    table = table[jax.random.permutation(jax.random.fold_in(own, 1), rows)]
    rotation = jax.random.randint(jax.random.fold_in(own, 2), (rows, 1), 0, top)
    return jnp.take_along_axis(table, (jnp.arange(top)[None, :] + rotation) % top, axis=1)


def load_shares(amount, total, most, slope, full):
    weights = [(1 << 20) // math.isqrt(grade ** slope) + 1 for grade in range(1, amount + 1)]
    largest = most if full else min(most, max(-(-total // amount), total * weights[0] // sum(weights)))
    least = 1 if total - largest >= amount - 1 else 0
    counts, rest = [largest] + [least] * (amount - 1), total - largest - least * (amount - 1)
    while rest > 0:
        movable = [i for i in range(1, amount) if counts[i] < largest] or [i for i in range(1, amount) if counts[i] < most]
        pool, budget = sum([weights[i] for i in movable]), rest
        for i in movable:
            extra = min(most - counts[i], max(1, budget * weights[i] // pool), rest)
            counts[i] = counts[i] + extra
            rest = rest - extra
    return np.array(counts)


def noise(own_key, shape, deviation, limit, pieces=(), kind=jnp.bfloat16):
    entries = jax.random.normal(own_key, shape, jnp.float32) * deviation
    if len(pieces) > 0:
        entries = block_scale(own_key, shape, pieces, -0.22, 0.18) * entries
    return jnp.clip(entries, min=-limit, max=limit).astype(kind)


def setup_inputs(seed: int = 0) -> dict:
    arg_keys = jax.random.split(jax.random.key(seed), 14)
    queries = draw_queries(jax.random.fold_in(arg_keys[13], 71), 0)
    keys = draw_keys(jax.random.fold_in(arg_keys[13], 71), 0)
    values = noise(arg_keys[2], (LEN, KVH * HD), 1.0, 6.0, ((0, 16),))
    query_gain = draw_query_gain(jax.random.fold_in(arg_keys[13], 71), 0)
    key_gain = draw_key_gain(jax.random.fold_in(arg_keys[13], 71), 0)
    out_weight = noise(arg_keys[5], (HQ * HD, D), (HD // 2) ** -0.5, 0.75, ((0, 16),))
    tokens_b = noise(arg_keys[6], (TOKB, D), 1.0, 6.0, ((0, 16),))
    norm_gain = jnp.clip(1.0 + 0.18 * jax.random.normal(arg_keys[7], (D,), jnp.float32), 0.1, 1.9)
    routes_keys = jax.random.split(jax.random.fold_in(arg_keys[8], 1), TOKB // TOK_DEV)
    routes_turns = jax.random.permutation(jax.random.fold_in(arg_keys[8], 3), TOKB // TOK_DEV)
    routes = jax.vmap(lambda own, number: deal_out(jax.random.fold_in(arg_keys[8], 2), own, number, TOK_DEV, EXPERTS, TOPK, CAP, 1))(routes_keys, routes_turns).reshape((TOKB, TOPK))
    route_weight = jnp.clip(jnp.exp(math.log(1.0) - 1.609438 * jax.random.uniform(arg_keys[9], (TOKB, TOPK), jnp.float32) ** block_scale(arg_keys[9], (TOKB, TOPK), ((0, 16),), -0.2, 0.2)), 0.2, 1.0)
    gate_weight = noise(arg_keys[10], (EXPERTS, D, FF), D ** -0.5, 0.125, ((0, 16), (2, 16)))
    up_weight = noise(arg_keys[11], (EXPERTS, D, FF), D ** -0.5, 0.125, ((0, 16), (2, 16)))
    down_weight = noise(arg_keys[12], (EXPERTS, FF, D), FF ** -0.5, 0.09375, ((0, 16), (1, 16)))
    return dict(queries=queries, keys=keys, values=values, query_gain=query_gain, key_gain=key_gain, out_weight=out_weight, tokens_b=tokens_b, norm_gain=norm_gain, routes=routes, route_weight=route_weight, gate_weight=gate_weight, up_weight=up_weight, down_weight=down_weight)


EPS = 1e-06
THETA = 10000.0
q_block = 64

def rotate(field, positions):
    n_freq = HD // 4
    row_pos = (positions // GRID_W).astype(jnp.float32)
    col_pos = (positions % GRID_W).astype(jnp.float32)
    inverse = THETA ** (-jnp.arange(n_freq, dtype=jnp.float32) / n_freq)
    angles = jnp.stack([row_pos[:, None] * inverse, col_pos[:, None] * inverse], axis=1)
    cosine = jnp.cos(angles)[:, None]
    sine = jnp.sin(angles)[:, None]
    length, n_heads = (field.shape[0], field.shape[1])
    halves = field.reshape(length, n_heads, 2, 2, n_freq)
    leading = halves[..., 0, :]
    second = halves[..., 1, :]
    turned = jnp.stack([leading * cosine - second * sine, second * cosine + leading * sine], axis=-2)
    return turned.reshape(length, n_heads, HD)

def prepare(source, gain_vec, positions, n_heads):
    length = source.shape[0]
    field = source.astype(jnp.float32).reshape(length, n_heads, HD)
    field = field * lax.rsqrt(lax.optimization_barrier(jnp.mean(field * field, axis=-1, keepdims=True)) + EPS) * gain_vec.astype(jnp.float32)
    return rotate(field, positions).astype(jnp.bfloat16)

def attend_block(query_blk, key_t, value_h):
    scores = jnp.einsum('qkgd,skd->kgqs', query_blk.astype(jnp.float32), key_t.astype(jnp.float32)) * HD ** (-0.5)
    row_max = lax.optimization_barrier(jnp.max(scores, axis=-1, keepdims=True))
    weights = jnp.exp(scores - row_max)
    totals = lax.optimization_barrier(jnp.sum(weights, axis=-1, keepdims=True))
    rounded = lax.optimization_barrier(weights.astype(jnp.bfloat16))
    merged = jnp.einsum('kgqs,skd->kgqd', rounded.astype(jnp.float32), value_h.astype(jnp.float32)) / totals
    return jnp.transpose(merged, (2, 0, 1, 3)).reshape(query_blk.shape[0], HQ * HD).astype(jnp.bfloat16)

def reference(queries, keys, values, query_gain, key_gain, out_weight, tokens_b, norm_gain, routes, route_weight, gate_weight, up_weight, down_weight):
    positions = jnp.arange(LEN, dtype=jnp.int32)
    query_t = prepare(queries, query_gain, positions, HQ).reshape(LEN // q_block, q_block, KVH, GROUP, HD)
    key_t = prepare(keys, key_gain, positions, KVH)
    value_h = values.reshape(LEN, KVH, HD)
    attended = lax.map(lambda query_blk: attend_block(query_blk, key_t, value_h), query_t).reshape(LEN, HQ * HD)
    mixed_out = jnp.dot(attended, out_weight, preferred_element_type=jnp.float32).astype(jnp.bfloat16)
    n_tokens = tokens_b.shape[0]
    n_blocks = n_tokens // TOK_DEV
    field = tokens_b.astype(jnp.float32)
    normed = (field * lax.rsqrt(lax.optimization_barrier(jnp.mean(field * field, axis=-1, keepdims=True)) + EPS) * norm_gain.astype(jnp.float32)).astype(jnp.bfloat16)
    assigned = routes.reshape(n_blocks, TOK_DEV * TOPK)
    onehot = (assigned[:, :, None] == jnp.arange(EXPERTS, dtype=jnp.int32)[None, None, :]).astype(jnp.int32)
    slot_rank = lax.optimization_barrier(jnp.sum((jnp.cumsum(onehot, axis=1) - onehot) * onehot, axis=-1))
    block_ids = jnp.arange(n_blocks, dtype=jnp.int32)[:, None]
    flat_slot = ((assigned * n_blocks + block_ids) * CAP + slot_rank).reshape(-1).astype(jnp.int32)
    row_ids = (block_ids * TOK_DEV + jnp.arange(TOK_DEV * TOPK, dtype=jnp.int32)[None, :] // TOPK).reshape(-1).astype(jnp.int32)
    slot_table = jnp.full((EXPERTS * n_blocks * CAP,), n_tokens, jnp.int32).at[flat_slot].set(row_ids)
    padded = jnp.concatenate([normed, jnp.zeros((1, D), jnp.bfloat16)], axis=0)
    width_part = FF // N_TP

    def expert_rows(stacked):
        row_index, gate_w, up_w, down_w = stacked
        inputs = padded[row_index].astype(jnp.float32)
        gate_act = jnp.einsum('nd,dtf->tnf', inputs, gate_w.reshape(D, N_TP, width_part).astype(jnp.float32))
        up_act = jnp.einsum('nd,dtf->tnf', inputs, up_w.reshape(D, N_TP, width_part).astype(jnp.float32))
        hidden = lax.optimization_barrier((jax.nn.silu(gate_act) * up_act).astype(jnp.bfloat16))
        partial_value = jnp.einsum('tnf,tfd->tnd', hidden.astype(jnp.float32), down_w.reshape(N_TP, width_part, D).astype(jnp.float32))
        partial_value = lax.optimization_barrier(partial_value.astype(jnp.bfloat16))
        return lax.optimization_barrier(jnp.sum(partial_value.astype(jnp.float32), axis=0)).astype(jnp.bfloat16)
    results = lax.map(expert_rows, (slot_table.reshape(EXPERTS, n_blocks * CAP), gate_weight, up_weight, down_weight))
    picked = results.reshape(-1, D)[flat_slot].astype(jnp.float32).reshape(n_tokens, TOPK, D)
    shares = route_weight / lax.optimization_barrier(jnp.sum(route_weight, axis=-1, keepdims=True))
    expert_out = lax.optimization_barrier(jnp.sum(shares[:, :, None] * picked, axis=1)).astype(jnp.bfloat16)
    return (mixed_out, expert_out)
```

```python
import functools
import math

import jax
import jax.numpy as jnp
from jax import lax
from jax.experimental import pallas as pl
from jax.experimental.pallas import tpu as pltpu
from jax.sharding import Mesh
from jax.sharding import PartitionSpec as P

D = 2048
HD = 128
HQ = 16
KVH = 4
FF_DEV = 256
CAP = 8
GRID_W = 64
EPS = 1e-06
THETA = 10000.0

NX = 4
NY = 4
NE = NX * NY
NZ = 8
ROWS = 768
TOK = 48
CH = NE * CAP
HALF = CH // 2

REACH = 3
DIRECT = [0] + list(range(REACH + 1, NZ - REACH))
SUBS = 2
RSUBS = 2

MESH = pl.DeviceIdType.MESH
F32 = jnp.float32
BF16 = jnp.bfloat16

PLACES = [(0, 0)]
PLACES += [(0, 3), (0, 1), (3, 0), (1, 0)]
PLACES += [(3, 3), (3, 1), (1, 3), (1, 1), (0, 2), (2, 0)]
PLACES += [(3, 2), (1, 2), (2, 3), (2, 1)]
PLACES += [(2, 2)]
SLOT = {place: i for i, place in enumerate(PLACES)}
KEYS_UNIT = 2 * ROWS
UNITS = NE * ROWS // KEYS_UNIT
Q_TILE = 128


def gather_messages():
    out = []
    for half in (0, 1):
        base = half * (ROWS // 2)
        full, quarter = ROWS // 2, ROWS // 4
        prim, sec = ("x", "y") if half == 0 else ("y", "x")

        def slot(p, s, half=half):
            p, s = p % 4, s % 4
            return SLOT[(s, p)] if half == 0 else SLOT[(p, s)]

        def send(level, axis, step, p, s, part, half=half, base=base, full=full, quarter=quarter,
                 prim=prim, sec=sec, slot=slot):
            tp, ts = (p - step, s) if axis == prim else (p, s - step)
            start = base + (quarter if part == 1 else 0)
            rows = full if part is None else quarter
            out.append((level, half, axis, step, slot(p, s), slot(tp, ts), start, rows))

        for axis in (prim, sec):
            for step in (1, -1):
                send(1, axis, step, 0, 0, None)
        for p, step, part in ((-1, 1, 0), (1, -1, 1)):
            send(2, prim, step, p, 0, part)
            send(2, sec, 1, p, 0, None)
            send(2, sec, -1, p, 0, None)
        send(2, sec, 1, 0, -1, 0)
        send(2, sec, -1, 0, 1, 1)
        for p in (-1, 1):
            send(3, sec, 1, p, -1, 0)
            send(3, sec, -1, p, 1, 1)
        send(3, sec, 1, 2, 0, None)
        send(3, sec, -1, 2, 0, None)
        send(4, sec, 1, 2, -1, 0)
        send(4, sec, -1, 2, 1, 1)
    return sorted(out, key=lambda m: m[0])


MESSAGES = gather_messages()
N_MSG = len(MESSAGES)


def body(
    q_hbm, k_hbm, v_hbm, qg_ref, kg_ref, cr_ref, sr_ref, cc_ref, sc_ref, ng_ref,
    r0_ref, r1_ref, w0_ref, w1_ref, tok_hbm, ow_hbm, wg_hbm, wu_hbm, wd_hbm,
    mixed_ref, expert_ref,
    q_buf, kv_raw, tok_buf, kv, q_n, m_ref, acc_ref, att, att_sib, slots, rows,
    wg, wu, wd, ow, part, rs_buf, ap, ars_buf, fin, ret, mat_ref,
    in_sem, d2d_send, d2d_recv, kv_send, kv_recv, kvd_send, kvd_recv,
    a2a_send, a2a_recv, z_send, z_recv, rs_send, rs_recv, ars_send, ars_recv,
    ret_send, ret_recv,
):
    y = lax.axis_index("y")
    x = lax.axis_index("x")
    z = lax.axis_index("z")
    c = lax.axis_index("c")
    me = y * NX + x
    sib = 1 - c

    def remote(src, dst, send_sem, recv_sem, **device):
        return pltpu.make_async_remote_copy(
            src_ref=src, dst_ref=dst, send_sem=send_sem, recv_sem=recv_sem,
            device_id=device, device_id_type=MESH,
        )

    head = (2 * z + c) // 4
    lane = pl.ds(pl.multiple_of(head * HD, HD), HD)
    loads = [
        pltpu.make_async_copy(k_hbm.at[:, lane], kv_raw, in_sem.at[0]),
        pltpu.make_async_copy(v_hbm.at[:, lane], kv.at[1, 0], in_sem.at[1]),
        pltpu.make_async_copy(q_hbm, q_buf, in_sem.at[2]),
    ]
    for i, delta in enumerate(DIRECT):
        blk = (z + delta) % NZ * 2 + c
        loads.append(
            pltpu.make_async_copy(
                tok_hbm.at[pl.ds(pl.multiple_of(blk * TOK, TOK), TOK), :],
                tok_buf.at[i], in_sem.at[3 + i],
            )
        )
    for copy in loads:
        copy.start()
    weights = []
    for i, (src, dst) in enumerate(((wg_hbm, wg), (wu_hbm, wu), (wd_hbm, wd), (ow_hbm, ow))):
        weights.append(pltpu.make_async_copy(src, dst.at[c], in_sem.at[3 + len(DIRECT) + i]))
    for copy in weights:
        copy.start()

    def make_slots(i):
        delta = DIRECT[i]
        blk = (z + delta) % NZ * 2 + c
        loads[3 + i].wait()
        field = tok_buf[i].astype(F32)
        scale = lax.rsqrt(jnp.mean(field * field, axis=1, keepdims=True) + EPS)
        normed = (field * scale * ng_ref[...]).astype(BF16)
        j = lax.broadcasted_iota(jnp.int32, (CH, TOK), 0)
        expert, rank = j // CAP, j % CAP
        r0 = r0_ref[pl.ds(blk, 1), :]
        r1 = r1_ref[pl.ds(blk, 1), :]
        hot = ((r0 == expert) | (r1 == expert)).astype(F32)
        before = (
            lax.broadcasted_iota(jnp.int32, (TOK, TOK), 0)
            < lax.broadcasted_iota(jnp.int32, (TOK, TOK), 1)
        ).astype(BF16)
        count = jnp.dot(hot.astype(BF16), before, preferred_element_type=F32)
        mat = jnp.where(count == rank.astype(F32), hot, 0.0)
        if i == 0:
            mat_ref[...] = mat
        slots[i] = jnp.dot(mat.astype(BF16), normed, preferred_element_type=F32).astype(
            BF16
        ).reshape(NE, CAP, D)

    def a2a(i, j):
        dy, dx = PLACES[j]
        ty, tx = (y + dy) % NY, (x + dx) % NX
        return remote(
            slots.at[i, ty * NX + tx], rows.at[(z + DIRECT[i]) % NZ, me],
            a2a_send.at[i, j], a2a_recv.at[i, j], y=ty, x=tx,
        )

    def start_direct(i):
        for j in range(1, NE):
            a2a(i, j).start()
        rows[(z + DIRECT[i]) % NZ, me] = slots[i, me]

    def wait_direct(i):
        for j in range(1, NE):
            a2a(i, j).wait_recv()

    make_slots(0)
    start_direct(0)

    lane_of = lax.broadcasted_iota(jnp.int32, (GRID_W, HD), 1)
    pi = lax.broadcasted_iota(jnp.int32, (HD, HD), 0)
    pj = lax.broadcasted_iota(jnp.int32, (HD, HD), 1)
    first_half = pj % 64 < 32
    swap = jnp.where(
        first_half & (pi == pj + 32), -1.0, jnp.where(~first_half & (pi == pj - 32), 1.0, 0.0)
    ).astype(BF16)

    def turn(src, gain_ref, factor, store):
        gain = gain_ref[...]
        other = jnp.where(
            lax.broadcasted_iota(jnp.int32, (1, HD), 1) % 64 < 32,
            pltpu.roll(gain, HD - 32, 1), pltpu.roll(gain, 32, 1),
        )
        for g in range(ROWS // GRID_W):
            raw = src[g * GRID_W : (g + 1) * GRID_W, :]
            val = raw.astype(F32)
            inv = lax.rsqrt(jnp.mean(val * val, axis=1, keepdims=True) + EPS)
            if factor != 1.0:
                inv = inv * factor
            turned = jnp.dot(raw, swap, preferred_element_type=F32)
            cosine = jnp.where(lane_of < 64, cr_ref[g : g + 1, :], cc_ref[...])
            sine = jnp.where(lane_of < 64, sr_ref[g : g + 1, :], sc_ref[...])
            store(g, ((val * (gain * cosine) + turned * (other * sine)) * inv).astype(BF16))

    def store_key(g, val):
        kv[0, 0, g * GRID_W : (g + 1) * GRID_W, :] = val

    def store_query(g, val):
        q_n[g * GRID_W : (g + 1) * GRID_W, :] = val

    loads[0].wait()
    turn(kv_raw, kg_ref, 1.0, store_key)
    loads[1].wait()

    def kv_copy(n):
        _, _, axis, step, src, dst, start, size = MESSAGES[n]
        here = y if axis == "y" else x
        span = pl.ds(start, size)
        return remote(
            kv.at[c, src, span], kv.at[c, dst, span], kv_send.at[n], kv_recv.at[n],
            **{axis: (here + step) % 4},
        )

    def kv_across(slot, half):
        n = (slot - 1) * 2 + half
        span = pl.ds(half * (ROWS // 2), ROWS // 2)
        return remote(
            kv.at[c, slot, span], kv.at[c, slot, span], kvd_send.at[n], kvd_recv.at[n], c=sib
        )

    def kv_await(slot, half):
        n = (slot - 1) * 2 + half
        span = pl.ds(half * (ROWS // 2), ROWS // 2)
        return remote(
            kv.at[sib, slot, span], kv.at[sib, slot, span], kvd_send.at[n], kvd_recv.at[n], c=sib
        )

    for n, msg in enumerate(MESSAGES):
        if msg[0] == 1:
            kv_copy(n).start()

    def kv_level(level):
        done = {}
        for n, msg in enumerate(MESSAGES):
            if msg[0] != level:
                continue
            _, half, _, _, _, dst, _, size = msg
            kv_copy(n).wait_recv()
            done[dst, half] = done.get((dst, half), 0) + size
            if done[dst, half] == ROWS // 2:
                for k, later in enumerate(MESSAGES):
                    if later[0] == level + 1 and later[1] == half and later[4] == dst:
                        kv_copy(k).start()
                kv_across(dst, half).start()

    loads[2].wait()
    turn(q_buf, qg_ref, HD ** (-0.5) * math.log2(math.e), store_query)

    pairs = [
        remote(buf.at[c], buf.at[c], d2d_send.at[i], d2d_recv.at[i], c=sib)
        for i, buf in enumerate((wg, wu, wd, ow))
    ]
    awaited = [
        remote(buf.at[sib], buf.at[sib], d2d_send.at[i], d2d_recv.at[i], c=sib)
        for i, buf in enumerate((wg, wu, wd, ow))
    ]

    for i in range(1, len(DIRECT)):
        make_slots(i)

    def z_copy(way, hop, sub):
        step = 1 if way == 0 else -1
        chunk = (z - step * hop) % NZ
        span = pl.ds(sub * (NE // SUBS), NE // SUBS)
        return remote(
            rows.at[chunk, span], rows.at[chunk, span],
            z_send.at[way, hop, sub], z_recv.at[way, hop, sub], z=(z + step) % NZ,
        )

    def z_wait(way, hop, sub):
        step = 1 if way == 0 else -1
        chunk = (z - step * (hop + 1)) % NZ
        span = pl.ds(sub * (NE // SUBS), NE // SUBS)
        return remote(
            rows.at[chunk, span], rows.at[chunk, span],
            z_send.at[way, hop, sub], z_recv.at[way, hop, sub], z=(z + step) % NZ,
        )

    def z_start():
        wait_direct(0)
        for sub in range(SUBS):
            for way in (0, 1):
                z_copy(way, 0, sub).start()

    def z_forward(hop, sub):
        for way in (0, 1):
            z_wait(way, hop, sub).wait_recv()
            if hop + 1 < REACH:
                z_copy(way, hop + 1, sub).start()

    m_ref[...] = jnp.full_like(m_ref, -1e30)
    acc_ref[...] = jnp.zeros_like(acc_ref)

    hops = [(hop, sub) for hop in range(REACH) for sub in range(SUBS)]
    plan = {u: [] for u in range(UNITS + 1)}
    plan[0] += [z_start, functools.partial(kv_level, 1)]
    plan[2] += [functools.partial(kv_level, 2)]
    plan[4] += [functools.partial(kv_level, 3)]
    plan[6] += [functools.partial(kv_level, 4)]

    def send_weights():
        for i in range(4):
            weights[i].wait()
            pairs[i].start()

    plan[1] += [send_weights]
    for i in range(1, len(DIRECT)):
        plan[5] += [functools.partial(start_direct, i)]
    for k, at in enumerate((3, 5, 7)):
        if k < len(hops):
            plan[at] += [functools.partial(z_forward, *hops[k])]
    for hop in hops[3:]:
        plan[UNITS] += [functools.partial(z_forward, *hop)]

    def unit(u, carry):
        for k in range(UNITS):
            @pl.when(u == k)
            def _(k=k):
                for act in plan[k]:
                    act()
                for slot in (2 * k, 2 * k + 1):
                    if slot > 0:
                        for half in (0, 1):
                            kv_await(slot, half).wait_recv()

        keys = kv[0, pl.ds(2 * u, 2)].reshape(KEYS_UNIT, HD)
        vals = kv[1, pl.ds(2 * u, 2)].reshape(KEYS_UNIT, HD)
        wide = jnp.concatenate([vals, jnp.ones_like(vals)], axis=1)
        for i in range(ROWS // Q_TILE):
            sl = pl.ds(i * Q_TILE, Q_TILE)
            s = lax.dot_general(
                q_n[sl, :], keys, (((1,), (1,)), ((), ())), preferred_element_type=F32
            )
            old = m_ref[sl, :]
            new = jnp.maximum(old, jnp.max(s, axis=1, keepdims=True))
            shrink = jnp.exp2(old - new)
            p = jnp.exp2(s - new[:, :1]).astype(BF16)
            acc_ref[sl, :] = acc_ref[sl, :] * jnp.concatenate([shrink, shrink], axis=1) + jnp.dot(
                p, wide, preferred_element_type=F32
            )
            m_ref[sl, :] = new
        return carry

    lax.fori_loop(0, UNITS, unit, 0)
    for t in range(2 * NZ):
        span = pl.ds(t * TOK, TOK)
        att[t % 2, t // 2] = (acc_ref[span, :HD] / acc_ref[span, HD:]).astype(BF16)
    swap_att = remote(att.at[sib], att_sib, d2d_send.at[4], d2d_recv.at[4], c=sib)
    swap_att.start()
    for act in plan[UNITS]:
        act()
    for i in range(1, len(DIRECT)):
        wait_direct(i)
    for copy in awaited:
        copy.wait_recv()
    swap_att.wait_recv()

    piece = HALF // RSUBS

    def rs_copy(way, s, u):
        step = 1 if way == 0 else -1
        return remote(
            rs_buf.at[way, s, u], rs_buf.at[way, s + 1, u],
            rs_send.at[way, s, u], rs_recv.at[way, s, u], z=(z + step) % NZ,
        )

    def ars_copy(way, s):
        step = 1 if way == 0 else -1
        return remote(
            ars_buf.at[way, s], ars_buf.at[way, s + 1],
            ars_send.at[way, s], ars_recv.at[way, s], z=(z + step) % NZ,
        )

    def ret_copy(e):
        return remote(
            fin.at[e], ret.at[me], ret_send.at[e], ret_recv.at[me], y=e // NX, x=e % NX
        )

    def rs_step(s, carry):
        chunk_r = (z - 1 - s + 2 * NZ) % NZ
        chunk_l = (z + 1 + s) % NZ
        act = jnp.concatenate(
            [
                rows[chunk_r, 0 : NE // 2].reshape(HALF, D),
                rows[chunk_l, NE // 2 : NE].reshape(HALF, D),
            ],
            axis=0,
        )
        hidden = []
        for k in range(2):
            gate = jnp.dot(act, wg[k], preferred_element_type=F32)
            up = jnp.dot(act, wu[k], preferred_element_type=F32)
            hidden.append((gate / (1.0 + jnp.exp(-gate)) * up).astype(BF16))
        for k in range(4):
            cols = pl.ds(k * (D // 4), D // 4)
            part[:, cols] = jnp.dot(hidden[0], wd[0, :, cols], preferred_element_type=F32) + jnp.dot(
                hidden[1], wd[1, :, cols], preferred_element_type=F32
            )
        for way, chunk in ((0, chunk_r), (1, chunk_l)):
            cols = pl.ds(way * (D // 2), D // 2)
            ap[way] = jnp.dot(att[c, chunk], ow[c, :, cols], preferred_element_type=F32) + jnp.dot(
                att_sib[chunk], ow[sib, :, cols], preferred_element_type=F32
            )

        for u in range(RSUBS):
            for way in (0, 1):
                span = pl.ds(way * HALF + u * piece, piece)

                @pl.when(s == 0)
                def _(way=way, u=u, span=span):
                    rs_buf[way, 0, u] = part[span, :].astype(BF16)
                    rs_copy(way, 0, u).start()

                @pl.when(s > 0)
                def _(way=way, u=u, span=span):
                    rs_copy(way, s - 1, u).wait_recv()
                    total = part[span, :] + rs_buf[way, s, u].astype(F32)

                    @pl.when(s < NZ - 1)
                    def _():
                        rs_buf[way, s, u] = total.astype(BF16)
                        rs_copy(way, s, u).start()

                    @pl.when(s == NZ - 1)
                    def _():
                        count = piece // CAP
                        first = way * (NE // 2) + u * count
                        fin[pl.ds(first, count)] = total.astype(BF16).reshape(count, CAP, D)
                        for e in range(first, first + count):
                            @pl.when(me != e)
                            def _(e=e):
                                ret_copy(e).start()

        for way in (0, 1):
            @pl.when(s == 0)
            def _(way=way):
                ars_buf[way, 0] = ap[way].astype(BF16)
                ars_copy(way, 0).start()

            @pl.when(s > 0)
            def _(way=way):
                ars_copy(way, s - 1).wait_recv()
                total = ap[way] + ars_buf[way, s].astype(F32)

                @pl.when(s < NZ - 1)
                def _():
                    ars_buf[way, s] = total.astype(BF16)
                    ars_copy(way, s).start()

                @pl.when(s == NZ - 1)
                def _():
                    mixed_ref[:, way * (D // 2) : (way + 1) * (D // 2)] = total.astype(BF16)

        return carry

    lax.fori_loop(0, NZ, rs_step, 0)

    ret[me] = fin[me]
    own = 2 * z + c
    j = lax.broadcasted_iota(jnp.int32, (CH, TOK), 0)
    w0 = w0_ref[pl.ds(own, 1), :]
    w1 = w1_ref[pl.ds(own, 1), :]
    share = jnp.where(r0_ref[pl.ds(own, 1), :] == j // CAP, w0, w1) / (w0 + w1)
    combine = jnp.where(mat_ref[...] > 0.5, share, 0.0)
    high = combine.astype(BF16)
    low = (combine - high.astype(F32)).astype(BF16)
    for e in range(NE):
        @pl.when(me != e)
        def _(e=e):
            remote(
                fin.at[e], ret.at[e], ret_send.at[e], ret_recv.at[e], y=e // NX, x=e % NX
            ).wait_recv()
    back = ret[...].reshape(CH, D)
    dims = (((0,), (0,)), ((), ()))
    expert_ref[...] = (
        lax.dot_general(high, back, dims, preferred_element_type=F32)
        + lax.dot_general(low, back, dims, preferred_element_type=F32)
    ).astype(BF16)

    for e in range(NE):
        @pl.when(me != e)
        def _(e=e):
            ret_copy(e).wait_send()
    for n in range(N_MSG):
        kv_copy(n).wait_send()
    for slot in range(1, NE):
        for half in (0, 1):
            kv_across(slot, half).wait_send()
    for i in range(len(DIRECT)):
        for k in range(1, NE):
            a2a(i, k).wait_send()
    for copy in pairs:
        copy.wait_send()
    swap_att.wait_send()
    for way in (0, 1):
        for hop, sub in hops:
            z_copy(way, hop, sub).wait_send()
        for s in range(NZ - 1):
            for u in range(RSUBS):
                rs_copy(way, s, u).wait_send()
            ars_copy(way, s).wait_send()


def fused(*args):
    vmem = pl.BlockSpec(memory_space=pltpu.VMEM)
    hbm = pl.BlockSpec(memory_space=pl.ANY)
    dma = pltpu.SemaphoreType.DMA
    n_direct = len(DIRECT)
    return pl.pallas_call(
        body,
        name="fused_step",
        out_shape=(
            jax.ShapeDtypeStruct((TOK, D), BF16),
            jax.ShapeDtypeStruct((TOK, D), BF16),
        ),
        in_specs=[hbm] * 3 + [vmem] * 11 + [hbm] * 5,
        out_specs=(vmem, vmem),
        scratch_shapes=[
            pltpu.VMEM((ROWS, HD), BF16),
            pltpu.VMEM((ROWS, HD), BF16),
            pltpu.VMEM((n_direct, TOK, D), BF16),
            pltpu.VMEM((2, NE, ROWS, HD), BF16),
            pltpu.VMEM((ROWS, HD), BF16),
            pltpu.VMEM((ROWS, HD), F32),
            pltpu.VMEM((ROWS, 2 * HD), F32),
            pltpu.VMEM((2, NZ, TOK, HD), BF16),
            pltpu.VMEM((NZ, TOK, HD), BF16),
            pltpu.VMEM((n_direct, NE, CAP, D), BF16),
            pltpu.VMEM((NZ, NE, CAP, D), BF16),
            pltpu.VMEM((2, D, FF_DEV), BF16),
            pltpu.VMEM((2, D, FF_DEV), BF16),
            pltpu.VMEM((2, FF_DEV, D), BF16),
            pltpu.VMEM((2, HD, D), BF16),
            pltpu.VMEM((CH, D), F32),
            pltpu.VMEM((2, NZ, RSUBS, HALF // RSUBS, D), BF16),
            pltpu.VMEM((2, TOK, D // 2), F32),
            pltpu.VMEM((2, NZ, TOK, D // 2), BF16),
            pltpu.VMEM((NE, CAP, D), BF16),
            pltpu.VMEM((NE, CAP, D), BF16),
            pltpu.VMEM((CH, TOK), F32),
            dma((3 + n_direct + 4,)),
            dma((5,)), dma((5,)),
            dma((N_MSG,)), dma((N_MSG,)),
            dma((2 * NE - 2,)), dma((2 * NE - 2,)),
            dma((n_direct, NE)), dma((n_direct, NE)),
            dma((2, REACH, SUBS)), dma((2, REACH, SUBS)),
            dma((2, NZ, RSUBS)), dma((2, NZ, RSUBS)),
            dma((2, NZ)), dma((2, NZ)),
            dma((NE,)), dma((NE,)),
        ],
        compiler_params=pltpu.CompilerParams(
            has_side_effects=True, vmem_limit_bytes=60 * 2**20
        ),
    )(*args)


def on_device(
    queries, keys, values, query_gain, key_gain, out_weight, tokens_b, norm_gain,
    routes, route_weight, gate_weight, up_weight, down_weight,
):
    n_freq = HD // 4
    lane = jnp.arange(HD, dtype=jnp.int32) % n_freq
    inverse = (THETA ** (-jnp.arange(n_freq, dtype=F32) / n_freq))[lane][None, :]
    ep = lax.axis_index("y") * NX + lax.axis_index("x")
    grid_rows = ROWS // GRID_W
    row_pos = (ep * grid_rows + jnp.arange(grid_rows, dtype=jnp.int32)).astype(F32)[:, None]
    col_pos = jnp.arange(GRID_W, dtype=jnp.int32).astype(F32)[:, None]
    by_row, by_col = row_pos * inverse, col_pos * inverse
    blocks = 2 * NZ
    picks = jnp.moveaxis(routes.reshape(blocks, TOK, 2), 2, 0)
    sizes = jnp.moveaxis(route_weight.reshape(blocks, TOK, 2), 2, 0)
    return fused(
        queries, keys, values, query_gain[None, :], key_gain[None, :],
        jnp.cos(by_row), jnp.sin(by_row), jnp.cos(by_col), jnp.sin(by_col),
        norm_gain[None, :], picks[0], picks[1], sizes[0], sizes[1], tokens_b,
        out_weight, gate_weight[0], up_weight[0], down_weight[0],
    )


def solution(mesh):
    torus = Mesh(mesh.devices.reshape(NY, NX, NZ, 2), ("y", "x", "z", "c"))
    ep, tp = ("y", "x"), ("z", "c")
    in_specs = (
        P(ep, tp), P(ep, None), P(ep, None), P(), P(), P(tp, None), P(ep, None), P(),
        P(ep, None), P(ep, None), P(ep, None, tp), P(ep, None, tp), P(ep, tp, None),
    )
    out_specs = (P(ep + tp, None), P(ep + tp, None))
    return jax.shard_map(
        on_device, mesh=torus, in_specs=in_specs, out_specs=out_specs, check_vma=False
    )
```

```python
import functools
import math

import jax
import jax.numpy as jnp
import numpy as np
from jax import lax
from jax.experimental import pallas as pl
from jax.experimental.pallas import tpu as pltpu
from jax.sharding import Mesh
from jax.sharding import PartitionSpec as P

D = 2048
HD = 128
HQ = 16
KVH = 4
FF_DEV = 256
CAP = 8
GRID_W = 64
EPS = 1e-06
THETA = 10000.0

NX = 4
NY = 4
NE = NX * NY
NZ = 8
ROWS = 768
TOK = 48
CH = NE * CAP
HALF = CH // 2

REACH = 2
DIRECT = [0] + list(range(REACH + 1, NZ - REACH))
SUBS = 2
RSUBS = 2

OWNERS = [(0, 2), (1, 2), (2, 0), (2, 1), (0, 0), (0, 1), (1, 0), (1, 1)]
OWNERS += [(2, 2), (2, 3), (3, 1), (3, 2), (0, 3), (3, 0), (3, 3), (1, 3)]
SELF = OWNERS.index((0, 0))
OTHERS = [p for p in range(NE) if p != SELF]

MESH = pl.DeviceIdType.MESH
F32 = jnp.float32
BF16 = jnp.bfloat16

PLACES = [(0, 0)]
PLACES += [(0, 3), (0, 1), (3, 0), (1, 0)]
PLACES += [(3, 3), (3, 1), (1, 3), (1, 1), (0, 2), (2, 0)]
PLACES += [(3, 2), (1, 2), (2, 3), (2, 1)]
PLACES += [(2, 2)]
SLOT = {place: i for i, place in enumerate(PLACES)}
KEYS_UNIT = 2 * ROWS
UNITS = NE * ROWS // KEYS_UNIT
EARLY = 6
Q_TILE = 128


def gather_messages():
    out = []
    for half in (0, 1):
        base = half * (ROWS // 2)
        full, quarter = ROWS // 2, ROWS // 4
        prim, sec = ("x", "y") if half == 0 else ("y", "x")

        def slot(p, s, half=half):
            p, s = p % 4, s % 4
            return SLOT[(s, p)] if half == 0 else SLOT[(p, s)]

        def send(level, axis, step, p, s, part, half=half, base=base, full=full, quarter=quarter,
                 prim=prim, sec=sec, slot=slot):
            tp, ts = (p - step, s) if axis == prim else (p, s - step)
            start = base + (quarter if part == 1 else 0)
            rows = full if part is None else quarter
            out.append((level, half, axis, step, slot(p, s), slot(tp, ts), start, rows))

        for axis in (prim, sec):
            for step in (1, -1):
                send(1, axis, step, 0, 0, None)
        for p, step, part in ((-1, 1, 0), (1, -1, 1)):
            send(2, prim, step, p, 0, part)
            send(2, sec, 1, p, 0, None)
            send(2, sec, -1, p, 0, None)
        send(2, sec, 1, 0, -1, 0)
        send(2, sec, -1, 0, 1, 1)
        for p in (-1, 1):
            send(3, sec, 1, p, -1, 0)
            send(3, sec, -1, p, 1, 1)
        send(3, sec, 1, 2, 0, None)
        send(3, sec, -1, 2, 0, None)
        send(4, sec, 1, 2, -1, 0)
        send(4, sec, -1, 2, 1, 1)
    return sorted(out, key=lambda m: m[0])


MESSAGES = gather_messages()
N_MSG = len(MESSAGES)


def body(
    q_hbm, k_hbm, v_hbm, qg_ref, kg_ref, inv_ref, ng_ref, routes_ref, sizes_ref,
    tok_hbm, ow_hbm, wg_hbm, wu_hbm, wd_hbm,
    out_ref,
    q_buf, kv_raw, tok_buf, kv, q_n, m_ref, acc_ref, att, att_sib, slots, rows,
    wg, wu, wd, ow, part, rs_buf, ap, ars_buf, fin, ret, mat_ref,
    in_sem, d2d_send, d2d_recv, kv_send, kv_recv, kvd_send, kvd_recv,
    a2a_send, a2a_recv, z_send, z_recv, rs_send, rs_recv, ars_send, ars_recv,
    ret_send, ret_recv,
):
    y = lax.axis_index("y")
    x = lax.axis_index("x")
    z = lax.axis_index("z")
    c = lax.axis_index("c")
    me = y * NX + x
    sib = 1 - c

    def remote(src, dst, send_sem, recv_sem, **device):
        return pltpu.make_async_remote_copy(
            src_ref=src, dst_ref=dst, send_sem=send_sem, recv_sem=recv_sem,
            device_id=device, device_id_type=MESH,
        )

    barrier = pltpu.get_barrier_semaphore()
    partners = [{"y": (y + dy) % NY, "x": (x + dx) % NX} for dy, dx in PLACES[1:]]
    partners += [{"z": (z + 1) % NZ}, {"z": (z + NZ - 1) % NZ}, {"c": sib}]
    for partner in partners:
        pl.semaphore_signal(barrier, inc=1, device_id=partner, device_id_type=MESH)

    head = (2 * z + c) // 4
    lane = pl.ds(pl.multiple_of(head * HD, HD), HD)
    loads = [
        pltpu.make_async_copy(k_hbm.at[:, lane], kv_raw, in_sem.at[0]),
        pltpu.make_async_copy(v_hbm.at[:, lane], kv.at[1, 0], in_sem.at[1]),
        pltpu.make_async_copy(q_hbm, q_buf, in_sem.at[2]),
    ]
    for i, delta in enumerate(DIRECT):
        blk = (z + delta) % NZ * 2 + c
        loads.append(
            pltpu.make_async_copy(
                tok_hbm.at[pl.ds(pl.multiple_of(blk * TOK, TOK), TOK), :],
                tok_buf.at[i], in_sem.at[3 + i],
            )
        )
    for copy in loads:
        copy.start()
    weights = []
    for i, (src, dst) in enumerate(((wg_hbm, wg), (wu_hbm, wu), (wd_hbm, wd), (ow_hbm, ow))):
        weights.append(pltpu.make_async_copy(src, dst.at[c], in_sem.at[3 + len(DIRECT) + i]))
    for copy in weights:
        copy.start()

    def block_of(ref, blk):
        return pltpu.roll(ref[...], (ROWS - blk * TOK) % ROWS, 1)[:, :TOK]

    def make_slots(i):
        delta = DIRECT[i]
        blk = (z + delta) % NZ * 2 + c
        loads[3 + i].wait()
        field = tok_buf[i].astype(F32)
        scale = lax.rsqrt(jnp.mean(field * field, axis=1, keepdims=True) + EPS)
        normed = (field * scale * ng_ref[...]).astype(BF16)
        j = lax.broadcasted_iota(jnp.int32, (CH, TOK), 0)
        expert, rank = j // CAP, j % CAP
        picks = block_of(routes_ref, blk)
        r0, r1 = picks[0:1], picks[1:2]
        hot = ((r0 == expert) | (r1 == expert)).astype(F32)
        before = (
            lax.broadcasted_iota(jnp.int32, (TOK, TOK), 0)
            < lax.broadcasted_iota(jnp.int32, (TOK, TOK), 1)
        ).astype(BF16)
        count = jnp.dot(hot.astype(BF16), before, preferred_element_type=F32)
        mat = jnp.where(count == rank.astype(F32), hot, 0.0)
        if i == 0:
            mat_ref[...] = mat
        slots[i] = jnp.dot(mat.astype(BF16), normed, preferred_element_type=F32).astype(
            BF16
        ).reshape(NE, CAP, D)

    def a2a(i, p):
        dy, dx = OWNERS[p]
        ty, tx = (y - dy + NY) % NY, (x - dx + NX) % NX
        return remote(
            slots.at[i, ty * NX + tx], rows.at[(z + DIRECT[i]) % NZ, p],
            a2a_send.at[i, p], a2a_recv.at[i, p], y=ty, x=tx,
        )

    def start_direct(i):
        for p in OTHERS:
            a2a(i, p).start()
        rows[(z + DIRECT[i]) % NZ, SELF] = slots[i, me]

    def wait_direct(i, first=0, last=NE):
        for p in OTHERS:
            if first <= p < last:
                a2a(i, p).wait_recv()

    make_slots(0)
    pl.semaphore_wait(barrier, len(partners))
    start_direct(0)

    lane_of = lax.broadcasted_iota(jnp.int32, (GRID_W, HD), 1)
    pi = lax.broadcasted_iota(jnp.int32, (HD, HD), 0)
    pj = lax.broadcasted_iota(jnp.int32, (HD, HD), 1)
    first_half = pj % 64 < 32
    swap = jnp.where(
        first_half & (pi == pj + 32), -1.0, jnp.where(~first_half & (pi == pj - 32), 1.0, 0.0)
    ).astype(BF16)

    row_pos = me * (ROWS // GRID_W) + lax.broadcasted_iota(jnp.int32, (16, HD), 0)
    col_pos = lax.broadcasted_iota(jnp.int32, (GRID_W, HD), 0)
    by_row = row_pos.astype(F32) * inv_ref[...]
    by_col = col_pos.astype(F32) * inv_ref[...]
    cos_row, sin_row = jnp.cos(by_row), jnp.sin(by_row)
    cos_col, sin_col = jnp.cos(by_col), jnp.sin(by_col)

    def turn(src, gain_ref, factor, store):
        gain = gain_ref[...]
        other = jnp.where(
            lax.broadcasted_iota(jnp.int32, (1, HD), 1) % 64 < 32,
            pltpu.roll(gain, HD - 32, 1), pltpu.roll(gain, 32, 1),
        )
        for g in range(ROWS // GRID_W):
            raw = src[g * GRID_W : (g + 1) * GRID_W, :]
            val = raw.astype(F32)
            inv = lax.rsqrt(jnp.mean(val * val, axis=1, keepdims=True) + EPS)
            if factor != 1.0:
                inv = inv * factor
            turned = jnp.dot(raw, swap, preferred_element_type=F32)
            cosine = jnp.where(lane_of < 64, cos_row[g : g + 1, :], cos_col)
            sine = jnp.where(lane_of < 64, sin_row[g : g + 1, :], sin_col)
            store(g, ((val * (gain * cosine) + turned * (other * sine)) * inv).astype(BF16))

    def store_key(g, val):
        kv[0, 0, g * GRID_W : (g + 1) * GRID_W, :] = val

    def store_query(g, val):
        q_n[g * GRID_W : (g + 1) * GRID_W, :] = val

    loads[0].wait()
    turn(kv_raw, kg_ref, 1.0, store_key)
    loads[1].wait()

    def kv_copy(n):
        _, _, axis, step, src, dst, start, size = MESSAGES[n]
        here = y if axis == "y" else x
        span = pl.ds(start, size)
        return remote(
            kv.at[c, src, span], kv.at[c, dst, span], kv_send.at[n], kv_recv.at[n],
            **{axis: (here + step) % 4},
        )

    def kv_across(slot, half):
        n = (slot - 1) * 2 + half
        span = pl.ds(half * (ROWS // 2), ROWS // 2)
        return remote(
            kv.at[c, slot, span], kv.at[c, slot, span], kvd_send.at[n], kvd_recv.at[n], c=sib
        )

    def kv_await(slot, half):
        n = (slot - 1) * 2 + half
        span = pl.ds(half * (ROWS // 2), ROWS // 2)
        return remote(
            kv.at[sib, slot, span], kv.at[sib, slot, span], kvd_send.at[n], kvd_recv.at[n], c=sib
        )

    for n, msg in enumerate(MESSAGES):
        if msg[0] == 1:
            kv_copy(n).start()

    def kv_level(level):
        done = {}
        for n, msg in enumerate(MESSAGES):
            if msg[0] != level:
                continue
            _, half, _, _, _, dst, _, size = msg
            kv_copy(n).wait_recv()
            done[dst, half] = done.get((dst, half), 0) + size
            if done[dst, half] == ROWS // 2:
                for k, later in enumerate(MESSAGES):
                    if later[0] == level + 1 and later[1] == half and later[4] == dst:
                        kv_copy(k).start()
                kv_across(dst, half).start()

    loads[2].wait()
    turn(q_buf, qg_ref, HD ** (-0.5) * math.log2(math.e), store_query)

    pairs = [
        remote(buf.at[c], buf.at[c], d2d_send.at[i], d2d_recv.at[i], c=sib)
        for i, buf in enumerate((wg, wu, wd, ow))
    ]
    awaited = [
        remote(buf.at[sib], buf.at[sib], d2d_send.at[i], d2d_recv.at[i], c=sib)
        for i, buf in enumerate((wg, wu, wd, ow))
    ]

    for i in range(1, len(DIRECT)):
        make_slots(i)

    def z_copy(way, hop, sub):
        step = 1 if way == 0 else -1
        chunk = (z - step * hop) % NZ
        span = pl.ds(sub * (NE // SUBS), NE // SUBS)
        return remote(
            rows.at[chunk, span], rows.at[chunk, span],
            z_send.at[way, hop, sub], z_recv.at[way, hop, sub], z=(z + step) % NZ,
        )

    def z_wait(way, hop, sub):
        step = 1 if way == 0 else -1
        chunk = (z - step * (hop + 1)) % NZ
        span = pl.ds(sub * (NE // SUBS), NE // SUBS)
        return remote(
            rows.at[chunk, span], rows.at[chunk, span],
            z_send.at[way, hop, sub], z_recv.at[way, hop, sub], z=(z + step) % NZ,
        )

    def z_start():
        for sub in range(SUBS):
            wait_direct(0, sub * (NE // SUBS), (sub + 1) * (NE // SUBS))
            for way in (0, 1):
                z_copy(way, 0, sub).start()

    def z_forward(hop, sub):
        for way in (0, 1):
            z_wait(way, hop, sub).wait_recv()
            if hop + 1 < REACH:
                z_copy(way, hop + 1, sub).start()

    m_ref[...] = jnp.full_like(m_ref, -1e30)
    acc_ref[...] = jnp.zeros_like(acc_ref)

    hops = [(hop, sub) for hop in range(REACH) for sub in range(SUBS)]
    plan = {u: [] for u in range(UNITS + 1)}
    plan[0] += [z_start, functools.partial(kv_level, 1)]
    def send_weights():
        for i in range(4):
            weights[i].wait()
            pairs[i].start()

    plan[1] += [send_weights]
    plan[2] += [
        functools.partial(z_forward, 0, 0), functools.partial(kv_level, 2),
        functools.partial(z_forward, 0, 1),
    ]
    plan[4] += [functools.partial(kv_level, 3)]
    plan[4] += [functools.partial(start_direct, i) for i in (1, 3)]
    plan[6] += [functools.partial(kv_level, 4), functools.partial(start_direct, 2)]

    def unit(u):
        for k in range(UNITS):
            @pl.when(u == k)
            def _(k=k):
                for act in plan[k]:
                    act()
                for slot in (2 * k, 2 * k + 1):
                    if slot > 0:
                        for half in (0, 1):
                            kv_await(slot, half).wait_recv()

        keys = kv[0, pl.ds(2 * u, 2)].reshape(KEYS_UNIT, HD)
        vals = kv[1, pl.ds(2 * u, 2)].reshape(KEYS_UNIT, HD)
        wide = jnp.concatenate([vals, jnp.ones_like(vals)], axis=1)
        for i in range(ROWS // Q_TILE):
            sl = pl.ds(i * Q_TILE, Q_TILE)
            s = lax.dot_general(
                q_n[sl, :], keys, (((1,), (1,)), ((), ())), preferred_element_type=F32
            )
            old = m_ref[sl, :]
            new = jnp.maximum(old, jnp.max(s, axis=1, keepdims=True))
            shrink = jnp.exp2(old - new)
            p = jnp.exp2(s - new[:, :1]).astype(BF16)
            acc_ref[sl, :] = acc_ref[sl, :] * jnp.concatenate([shrink, shrink], axis=1) + jnp.dot(
                p, wide, preferred_element_type=F32
            )
            m_ref[sl, :] = new

    swap_att = remote(att.at[sib], att_sib, d2d_send.at[4], d2d_recv.at[4], c=sib)

    def finish_attention():
        for t in range(2 * NZ):
            span = pl.ds(t * TOK, TOK)
            att[t % 2, t // 2] = (acc_ref[span, :HD] / acc_ref[span, HD:]).astype(BF16)
        swap_att.start()

    piece = HALF // RSUBS

    def rs_copy(way, s, u):
        step = 1 if way == 0 else -1
        return remote(
            rs_buf.at[way, s, u], rs_buf.at[way, s + 1, u],
            rs_send.at[way, s, u], rs_recv.at[way, s, u], z=(z + step) % NZ,
        )

    def ars_copy(way, s):
        step = 1 if way == 0 else -1
        return remote(
            ars_buf.at[way, s], ars_buf.at[way, s + 1],
            ars_send.at[way, s], ars_recv.at[way, s], z=(z + step) % NZ,
        )

    def ret_copy(p):
        dy, dx = OWNERS[p]
        return remote(
            fin.at[p], ret.at[me], ret_send.at[p], ret_recv.at[p],
            y=(y + dy) % NY, x=(x + dx) % NX,
        )

    def moe_step(s):
        for k in range(NZ // 2):
            @pl.when(s == k)
            def _(k=k):
                if k == 0:
                    for copy in awaited:
                        copy.wait_recv()
                elif k < REACH:
                    for sub in range(SUBS):
                        z_forward(k, sub)
                else:
                    for delta in sorted({k + 1, NZ - k - 1}):
                        wait_direct(DIRECT.index(delta))

        chunk_r = (z - 1 - s + 2 * NZ) % NZ
        chunk_l = (z + 1 + s) % NZ
        act = jnp.concatenate(
            [
                rows[chunk_r, 0 : NE // 2].reshape(HALF, D),
                rows[chunk_l, NE // 2 : NE].reshape(HALF, D),
            ],
            axis=0,
        )
        hidden = []
        for k in range(2):
            gate = jnp.dot(act, wg[k], preferred_element_type=F32)
            up = jnp.dot(act, wu[k], preferred_element_type=F32)
            hidden.append((gate / (1.0 + jnp.exp(-gate)) * up).astype(BF16))
        for k in range(4):
            cols = pl.ds(k * (D // 4), D // 4)
            part[:, cols] = jnp.dot(hidden[0], wd[0, :, cols], preferred_element_type=F32) + jnp.dot(
                hidden[1], wd[1, :, cols], preferred_element_type=F32
            )
        for u in range(RSUBS):
            for way in (0, 1):
                span = pl.ds(way * HALF + u * piece, piece)

                @pl.when(s == 0)
                def _(way=way, u=u, span=span):
                    rs_buf[way, 0, u] = part[span, :].astype(BF16)
                    rs_copy(way, 0, u).start()

                @pl.when(s > 0)
                def _(way=way, u=u, span=span):
                    rs_copy(way, s - 1, u).wait_recv()
                    total = part[span, :] + rs_buf[way, s, u].astype(F32)

                    @pl.when(s < NZ - 1)
                    def _():
                        rs_buf[way, s, u] = total.astype(BF16)
                        rs_copy(way, s, u).start()

                    @pl.when(s == NZ - 1)
                    def _():
                        count = piece // CAP
                        first = way * (NE // 2) + u * count
                        fin[pl.ds(first, count)] = total.astype(BF16).reshape(count, CAP, D)
                        for p in range(first, first + count):
                            if p != SELF:
                                ret_copy(p).start()

    def att_step(s):
        @pl.when(s == 0)
        def _():
            swap_att.wait_recv()

        chunk_r = (z - 1 - s + 2 * NZ) % NZ
        chunk_l = (z + 1 + s) % NZ
        for way, chunk in ((0, chunk_r), (1, chunk_l)):
            cols = pl.ds(way * (D // 2), D // 2)
            ap[way] = jnp.dot(att[c, chunk], ow[c, :, cols], preferred_element_type=F32) + jnp.dot(
                att_sib[chunk], ow[sib, :, cols], preferred_element_type=F32
            )

        for way in (0, 1):
            @pl.when(s == 0)
            def _(way=way):
                ars_buf[way, 0] = ap[way].astype(BF16)
                ars_copy(way, 0).start()

            @pl.when(s > 0)
            def _(way=way):
                ars_copy(way, s - 1).wait_recv()
                total = ap[way] + ars_buf[way, s].astype(F32)

                @pl.when(s < NZ - 1)
                def _():
                    ars_buf[way, s] = total.astype(BF16)
                    ars_copy(way, s).start()

                @pl.when(s == NZ - 1)
                def _():
                    out_ref[0, :, way * (D // 2) : (way + 1) * (D // 2)] = total.astype(BF16)

    def tick(t, carry):
        @pl.when(t < UNITS)
        def _():
            unit(t)

        @pl.when(t == UNITS - 1)
        def _():
            finish_attention()

        @pl.when((t == EARLY) | ((t >= UNITS) & (t < UNITS + NZ - 1)))
        def _():
            moe_step(jnp.where(t == EARLY, 0, t - UNITS + 1))

        @pl.when(t >= UNITS)
        def _():
            att_step(t - UNITS)

        return carry

    lax.fori_loop(0, UNITS + NZ, tick, 0)

    ret[me] = fin[SELF]
    own = 2 * z + c
    j = lax.broadcasted_iota(jnp.int32, (CH, TOK), 0)
    picks = block_of(routes_ref, own)
    sizes = block_of(sizes_ref, own)
    w0, w1 = sizes[0:1], sizes[1:2]
    share = jnp.where(picks[0:1] == j // CAP, w0, w1) / (w0 + w1)
    combine = jnp.where(mat_ref[...] > 0.5, share, 0.0)
    high = combine.astype(BF16)
    low = (combine - high.astype(F32)).astype(BF16)
    for p in OTHERS:
        ret_copy(p).wait_recv()
    back = ret[...].reshape(CH, D)
    dims = (((0,), (0,)), ((), ()))
    out_ref[1] = (
        lax.dot_general(high, back, dims, preferred_element_type=F32)
        + lax.dot_general(low, back, dims, preferred_element_type=F32)
    ).astype(BF16)

    for p in OTHERS:
        ret_copy(p).wait_send()
    for n in range(N_MSG):
        kv_copy(n).wait_send()
    for slot in range(1, NE):
        for half in (0, 1):
            kv_across(slot, half).wait_send()
    for i in range(len(DIRECT)):
        for p in OTHERS:
            a2a(i, p).wait_send()
    for copy in pairs:
        copy.wait_send()
    swap_att.wait_send()
    for way in (0, 1):
        for hop, sub in hops:
            z_copy(way, hop, sub).wait_send()
        for s in range(NZ - 1):
            for u in range(RSUBS):
                rs_copy(way, s, u).wait_send()
            ars_copy(way, s).wait_send()


def fused(*args):
    vmem = pl.BlockSpec(memory_space=pltpu.VMEM)
    hbm = pl.BlockSpec(memory_space=pl.ANY)
    dma = pltpu.SemaphoreType.DMA
    n_direct = len(DIRECT)
    return pl.pallas_call(
        body,
        name="fused_step",
        out_shape=jax.ShapeDtypeStruct((2, TOK, D), BF16),
        in_specs=[hbm] * 3 + [vmem] * 6 + [hbm] * 5,
        out_specs=vmem,
        scratch_shapes=[
            pltpu.VMEM((ROWS, HD), BF16),
            pltpu.VMEM((ROWS, HD), BF16),
            pltpu.VMEM((n_direct, TOK, D), BF16),
            pltpu.VMEM((2, NE, ROWS, HD), BF16),
            pltpu.VMEM((ROWS, HD), BF16),
            pltpu.VMEM((ROWS, HD), F32),
            pltpu.VMEM((ROWS, 2 * HD), F32),
            pltpu.VMEM((2, NZ, TOK, HD), BF16),
            pltpu.VMEM((NZ, TOK, HD), BF16),
            pltpu.VMEM((n_direct, NE, CAP, D), BF16),
            pltpu.VMEM((NZ, NE, CAP, D), BF16),
            pltpu.VMEM((2, D, FF_DEV), BF16),
            pltpu.VMEM((2, D, FF_DEV), BF16),
            pltpu.VMEM((2, FF_DEV, D), BF16),
            pltpu.VMEM((2, HD, D), BF16),
            pltpu.VMEM((CH, D), F32),
            pltpu.VMEM((2, NZ, RSUBS, HALF // RSUBS, D), BF16),
            pltpu.VMEM((2, TOK, D // 2), F32),
            pltpu.VMEM((2, NZ, TOK, D // 2), BF16),
            pltpu.VMEM((NE, CAP, D), BF16),
            pltpu.VMEM((NE, CAP, D), BF16),
            pltpu.VMEM((CH, TOK), F32),
            dma((3 + n_direct + 4,)),
            dma((5,)), dma((5,)),
            dma((N_MSG,)), dma((N_MSG,)),
            dma((2 * NE - 2,)), dma((2 * NE - 2,)),
            dma((n_direct, NE)), dma((n_direct, NE)),
            dma((2, REACH, SUBS)), dma((2, REACH, SUBS)),
            dma((2, NZ, RSUBS)), dma((2, NZ, RSUBS)),
            dma((2, NZ)), dma((2, NZ)),
            dma((NE,)), dma((NE,)),
        ],
        compiler_params=pltpu.CompilerParams(
            collective_id=0, has_side_effects=True, vmem_limit_bytes=60 * 2**20
        ),
    )(*args)


def on_device(
    queries, keys, values, query_gain, key_gain, out_weight, tokens_b, norm_gain,
    routes, route_weight, gate_weight, up_weight, down_weight,
):
    n_freq = HD // 4
    inverse = np.tile(THETA ** (-np.arange(n_freq) / n_freq), HD // n_freq).astype(np.float32)
    both = fused(
        queries, keys, values, query_gain[None, :], key_gain[None, :], jnp.asarray(inverse)[None, :],
        norm_gain[None, :], routes.T, route_weight.T, tokens_b,
        out_weight, gate_weight[0], up_weight[0], down_weight[0],
    )
    return both[0], both[1]


def solution(mesh):
    torus = Mesh(mesh.devices.reshape(NY, NX, NZ, 2), ("y", "x", "z", "c"))
    ep, tp = ("y", "x"), ("z", "c")
    in_specs = (
        P(ep, tp), P(ep, None), P(ep, None), P(), P(), P(tp, None), P(ep, None), P(),
        P(ep, None), P(ep, None), P(ep, None, tp), P(ep, None, tp), P(ep, tp, None),
    )
    out_specs = (P(ep + tp, None), P(ep + tp, None))
    return jax.shard_map(
        on_device, mesh=torus, in_specs=in_specs, out_specs=out_specs, check_vma=False
    )
```

```python
import functools
import math

import jax
import jax.numpy as jnp
import numpy as np
from jax import lax
from jax.experimental import pallas as pl
from jax.experimental.pallas import tpu as pltpu
from jax.sharding import Mesh
from jax.sharding import PartitionSpec as P

D = 2048
HD = 128
HQ = 16
KVH = 4
FF_DEV = 256
CAP = 8
GRID_W = 64
EPS = 1e-06
THETA = 10000.0

NX = 4
NY = 4
NE = NX * NY
NZ = 8
ROWS = 768
TOK = 48
CH = NE * CAP
HALF = CH // 2

REACH = 2
DIRECT = [0] + list(range(REACH + 1, NZ - REACH))
SUBS = 4
PIECE = NE // SUBS
SUB_ORDER = (1, 3, 0, 2)
RSUBS = 2

OWNERS = [(0, 2), (1, 2), (2, 0), (2, 1), (0, 0), (0, 1), (1, 0), (1, 1)]
OWNERS += [(2, 2), (2, 3), (3, 1), (3, 2), (0, 3), (3, 0), (3, 3), (1, 3)]
SELF = OWNERS.index((0, 0))
OTHERS = [p for p in range(NE) if p != SELF]
NEAR_FIRST = [p for sub in SUB_ORDER for p in range(sub * PIECE, (sub + 1) * PIECE) if p != SELF]

MESH = pl.DeviceIdType.MESH
F32 = jnp.float32
BF16 = jnp.bfloat16

PLACES = [(0, 0)]
PLACES += [(0, 3), (0, 1), (3, 0), (1, 0)]
PLACES += [(3, 3), (3, 1), (1, 3), (1, 1), (0, 2), (2, 0)]
PLACES += [(3, 2), (1, 2), (2, 3), (2, 1)]
PLACES += [(2, 2)]
SLOT = {place: i for i, place in enumerate(PLACES)}
KEYS_UNIT = 2 * ROWS
UNITS = NE * ROWS // KEYS_UNIT
EARLY = (4, 6)
TICKS = UNITS + NZ - len(EARLY)
WO_ROWS = NZ * HD
Q_TILE = 128


def gather_messages():
    out = []
    for half in (0, 1):
        base = half * (ROWS // 2)
        full, quarter = ROWS // 2, ROWS // 4
        prim, sec = ("x", "y") if half == 0 else ("y", "x")

        def slot(p, s, half=half):
            p, s = p % 4, s % 4
            return SLOT[(s, p)] if half == 0 else SLOT[(p, s)]

        def send(level, axis, step, p, s, part, half=half, base=base, full=full, quarter=quarter,
                 prim=prim, sec=sec, slot=slot):
            tp, ts = (p - step, s) if axis == prim else (p, s - step)
            start = base + (quarter if part == 1 else 0)
            rows = full if part is None else quarter
            out.append((level, half, axis, step, slot(p, s), slot(tp, ts), start, rows))

        for axis in (prim, sec):
            for step in (1, -1):
                send(1, axis, step, 0, 0, None)
        for p, step, part in ((-1, 1, 0), (1, -1, 1)):
            send(2, prim, step, p, 0, part)
            send(2, sec, 1, p, 0, None)
            send(2, sec, -1, p, 0, None)
        send(2, sec, 1, 0, -1, 0)
        send(2, sec, -1, 0, 1, 1)
        for p in (-1, 1):
            send(3, sec, 1, p, -1, 0)
            send(3, sec, -1, p, 1, 1)
        send(3, sec, 1, 2, 0, None)
        send(3, sec, -1, 2, 0, None)
        send(4, sec, 1, 2, -1, 0)
        send(4, sec, -1, 2, 1, 1)
    return sorted(out, key=lambda m: m[0])


MESSAGES = gather_messages()
N_MSG = len(MESSAGES)


def body(
    q_hbm, k_hbm, v_hbm, qg_ref, kg_ref, inv_ref, ng_ref, routes_ref, sizes_ref,
    tok_hbm, ow_hbm, wg_hbm, wu_hbm, wd_hbm,
    out_ref,
    q_buf, kv_raw, tok_buf, kv, q_n, m_ref, acc_ref, att, slots, rows,
    wg, wu, wd, wo, att_all, part, rs_buf, fin, ret, mat_ref, comb, stage,
    in_sem, d2d_send, d2d_recv, sent, a2a_sent, ring_sent, kv_recv, kvd_recv, a2a_recv, z_recv,
    wo_recv, wod_recv, rs_recv, out_sem,
):
    y = lax.axis_index("y")
    x = lax.axis_index("x")
    z = lax.axis_index("z")
    c = lax.axis_index("c")
    me = y * NX + x
    sib = 1 - c

    def remote(src, dst, send_sem, recv_sem, **device):
        return pltpu.make_async_remote_copy(
            src_ref=src, dst_ref=dst, send_sem=send_sem, recv_sem=recv_sem,
            device_id=device, device_id_type=MESH,
        )

    barrier = pltpu.get_barrier_semaphore()
    partners = [{"y": (y + dy) % NY, "x": (x + dx) % NX} for dy, dx in PLACES[1:]]
    partners += [{"z": (z + dz) % NZ} for dz in range(1, NZ)]
    partners += [{"z": (z + dz) % NZ, "c": sib} for dz in range(NZ)]
    for partner in partners:
        pl.semaphore_signal(barrier, inc=1, device_id=partner, device_id_type=MESH)

    outs = [pltpu.make_async_copy(stage.at[i], out_ref.at[i], out_sem.at[i]) for i in range(2)]

    head = (2 * z + c) // 4
    lane = pl.ds(pl.multiple_of(head * HD, HD), HD)
    loads = [
        pltpu.make_async_copy(k_hbm.at[:, lane], kv_raw, in_sem.at[0]),
        pltpu.make_async_copy(v_hbm.at[:, lane], kv.at[1, 0], in_sem.at[1]),
        pltpu.make_async_copy(q_hbm, q_buf, in_sem.at[2]),
    ]
    for i, delta in enumerate(DIRECT):
        blk = (z + delta) % NZ * 2 + c
        loads.append(
            pltpu.make_async_copy(
                tok_hbm.at[pl.ds(pl.multiple_of(blk * TOK, TOK), TOK), :],
                tok_buf.at[i], in_sem.at[3 + i],
            )
        )
    for copy in loads:
        copy.start()
    weights = []
    for i, (src, dst) in enumerate(((wg_hbm, wg), (wu_hbm, wu), (wd_hbm, wd))):
        weights.append(pltpu.make_async_copy(src, dst.at[c], in_sem.at[3 + len(DIRECT) + i]))
    slab = pl.ds(pl.multiple_of(me * HD, HD), HD)
    wo_own = wo.at[c, 0, pl.ds(pl.multiple_of(z * HD, HD), HD)]
    wo_load = pltpu.make_async_copy(ow_hbm.at[:, slab], wo_own, in_sem.at[6 + len(DIRECT)])
    wo_load.start()
    for copy in weights:
        copy.start()

    def block_of(ref, blk):
        return pltpu.roll(ref[...], (ROWS - blk * TOK) % ROWS, 1)[:, :TOK]

    def make_slots(i):
        delta = DIRECT[i]
        blk = (z + delta) % NZ * 2 + c
        loads[3 + i].wait()
        field = tok_buf[i].astype(F32)
        scale = lax.rsqrt(jnp.mean(field * field, axis=1, keepdims=True) + EPS)
        normed = (field * scale * ng_ref[...]).astype(BF16)
        j = lax.broadcasted_iota(jnp.int32, (CH, TOK), 0)
        expert, rank = j // CAP, j % CAP
        picks = block_of(routes_ref, blk)
        r0, r1 = picks[0:1], picks[1:2]
        hot = ((r0 == expert) | (r1 == expert)).astype(F32)
        before = (
            lax.broadcasted_iota(jnp.int32, (TOK, TOK), 0)
            < lax.broadcasted_iota(jnp.int32, (TOK, TOK), 1)
        ).astype(BF16)
        count = jnp.dot(hot.astype(BF16), before, preferred_element_type=F32)
        mat = jnp.where(count == rank.astype(F32), hot, 0.0)
        if i == 0:
            mat_ref[...] = mat
        slots[i] = jnp.dot(mat.astype(BF16), normed, preferred_element_type=F32).astype(
            BF16
        ).reshape(NE, CAP, D)

    def a2a(i, p):
        dy, dx = OWNERS[p]
        ty, tx = (y - dy + NY) % NY, (x - dx + NX) % NX
        return remote(
            slots.at[i, ty * NX + tx], rows.at[(z + DIRECT[i]) % NZ, p],
            a2a_sent.at[i], a2a_recv.at[p // PIECE if i == 0 else SUBS + i - 1], y=ty, x=tx,
        )

    def start_direct(i):
        for p in NEAR_FIRST:
            a2a(i, p).start()
        rows[(z + DIRECT[i]) % NZ, SELF] = slots[i, me]

    def wait_rows(i, sem, first, count):
        span = rows.at[(z + DIRECT[i]) % NZ, pl.ds(first, count)]
        remote(span, span, a2a_sent.at[i], a2a_recv.at[sem], c=sib).wait_recv()

    def wait_own(sub):
        wait_rows(0, sub, sub * PIECE, PIECE - (SELF // PIECE == sub))

    def wait_direct(i):
        wait_rows(i, SUBS + i - 1, 0, NE - 1)

    make_slots(0)
    pl.semaphore_wait(barrier, len(partners))
    start_direct(0)

    own = 2 * z + c
    j = lax.broadcasted_iota(jnp.int32, (CH, TOK), 0)
    picks = block_of(routes_ref, own)
    sizes = block_of(sizes_ref, own)
    w0, w1 = sizes[0:1], sizes[1:2]
    share = jnp.where(picks[0:1] == j // CAP, w0, w1) / (w0 + w1)
    combine = jnp.where(mat_ref[...] > 0.5, share, 0.0)
    high = combine.astype(BF16)
    comb[0] = high
    comb[1] = (combine - high.astype(F32)).astype(BF16)

    lane_of = lax.broadcasted_iota(jnp.int32, (GRID_W, HD), 1)
    pi = lax.broadcasted_iota(jnp.int32, (HD, HD), 0)
    pj = lax.broadcasted_iota(jnp.int32, (HD, HD), 1)
    first_half = pj % 64 < 32
    swap = jnp.where(
        first_half & (pi == pj + 32), -1.0, jnp.where(~first_half & (pi == pj - 32), 1.0, 0.0)
    ).astype(BF16)

    row_pos = me * (ROWS // GRID_W) + lax.broadcasted_iota(jnp.int32, (16, HD), 0)
    col_pos = lax.broadcasted_iota(jnp.int32, (GRID_W, HD), 0)
    by_row = row_pos.astype(F32) * inv_ref[...]
    by_col = col_pos.astype(F32) * inv_ref[...]
    cos_row, sin_row = jnp.cos(by_row), jnp.sin(by_row)
    cos_col, sin_col = jnp.cos(by_col), jnp.sin(by_col)

    def turn(src, gain_ref, factor, store):
        gain = gain_ref[...]
        other = jnp.where(
            lax.broadcasted_iota(jnp.int32, (1, HD), 1) % 64 < 32,
            pltpu.roll(gain, HD - 32, 1), pltpu.roll(gain, 32, 1),
        )
        for g in range(ROWS // GRID_W):
            raw = src[g * GRID_W : (g + 1) * GRID_W, :]
            val = raw.astype(F32)
            inv = lax.rsqrt(jnp.mean(val * val, axis=1, keepdims=True) + EPS)
            if factor != 1.0:
                inv = inv * factor
            turned = jnp.dot(raw, swap, preferred_element_type=F32)
            cosine = jnp.where(lane_of < 64, cos_row[g : g + 1, :], cos_col)
            sine = jnp.where(lane_of < 64, sin_row[g : g + 1, :], sin_col)
            store(g, ((val * (gain * cosine) + turned * (other * sine)) * inv).astype(BF16))

    def store_key(g, val):
        kv[0, 0, g * GRID_W : (g + 1) * GRID_W, :] = val

    def store_query(g, val):
        q_n[g * GRID_W : (g + 1) * GRID_W, :] = val

    loads[0].wait()
    turn(kv_raw, kg_ref, 1.0, store_key)
    loads[1].wait()

    class Gather:
        def __init__(self, buf, size, first, arrived, crossed):
            self.buf, self.size, self.arrived, self.crossed = buf, size, arrived, crossed
            self.ring, self.across_sem = sent.at[first], sent.at[first + 1]

        def copy(self, n):
            _, half, axis, step, src, dst, start, count = MESSAGES[n]
            here = y if axis == "y" else x
            span = pl.ds(start * self.size // ROWS, count * self.size // ROWS)
            return remote(
                self.buf.at[c, src, span], self.buf.at[c, dst, span], self.ring,
                self.arrived.at[(dst - 1) * 2 + half], **{axis: (here + step) % 4},
            )

        def start(self):
            for n, msg in enumerate(MESSAGES):
                if msg[0] == 1:
                    self.copy(n).start()

        def level(self, level):
            for dst, half in dict.fromkeys((m[5], m[1]) for m in MESSAGES if m[0] == level):
                span = self.buf.at[c, dst, pl.ds(half * (self.size // 2), self.size // 2)]
                remote(span, span, self.ring, self.arrived.at[(dst - 1) * 2 + half], c=sib).wait_recv()
                for k, later in enumerate(MESSAGES):
                    if later[0] == level + 1 and later[1] == half and later[4] == dst:
                        self.copy(k).start()
                remote(span, span, self.across_sem, self.crossed.at[dst // 2], c=sib).start()

        def wait(self, pair):
            first = max(2 * pair, 1)
            span = self.buf.at[sib, pl.ds(first, 2 * pair + 2 - first)]
            remote(span, span, self.across_sem, self.crossed.at[pair], c=sib).wait_recv()

    kvs = Gather(kv, ROWS, 0, kv_recv, kvd_recv)
    wos = Gather(wo, WO_ROWS, 5, wo_recv, wod_recv)
    kv_level = kvs.level
    kvs.start()

    def wo_copy(dz):
        return remote(wo_own, wo_own, sent.at[7], sent.at[8], z=(z + dz) % NZ)

    wo_load.wait()
    for dz in range(1, NZ):
        wo_copy(dz).start()

    def wo_start():
        span = wo.at[c, 0, pl.ds(0, WO_ROWS - HD)]
        remote(span, span, sent.at[7], sent.at[8], c=sib).wait_recv()
        own = wo.at[c, 0]
        remote(own, own, d2d_send.at[3], d2d_recv.at[3], c=sib).start()
        wos.start()

    loads[2].wait()
    turn(q_buf, qg_ref, HD ** (-0.5) * math.log2(math.e), store_query)

    pairs = [
        remote(buf.at[c], buf.at[c], d2d_send.at[i], d2d_recv.at[i], c=sib)
        for i, buf in enumerate((wg, wu, wd))
    ]
    awaited = [
        remote(buf.at[sib], buf.at[sib], d2d_send.at[i], d2d_recv.at[i], c=sib)
        for i, buf in enumerate((wg, wu, wd))
    ]

    for i in range(1, len(DIRECT)):
        make_slots(i)

    def z_copy(way, hop, sub):
        step = 1 if way == 0 else -1
        chunk = (z - step * hop) % NZ
        span = pl.ds(sub * PIECE, PIECE)
        return remote(
            rows.at[chunk, span], rows.at[chunk, span],
            sent.at[2], z_recv.at[way, hop, sub], z=(z + step) % NZ,
        )

    def z_wait(way, hop, sub):
        step = 1 if way == 0 else -1
        chunk = (z - step * (hop + 1)) % NZ
        span = pl.ds(sub * PIECE, PIECE)
        return remote(
            rows.at[chunk, span], rows.at[chunk, span],
            sent.at[2], z_recv.at[way, hop, sub], z=(z + step) % NZ,
        )

    def z_start():
        for sub in SUB_ORDER:
            wait_own(sub)
            for way in (0, 1):
                z_copy(way, 0, sub).start()

    def z_forward(hop, sub):
        for way in (0, 1):
            z_wait(way, hop, sub).wait_recv()
            if hop + 1 < REACH:
                z_copy(way, hop + 1, sub).start()

    m_ref[...] = jnp.full_like(m_ref, -1e30)
    acc_ref[...] = jnp.zeros_like(acc_ref)

    hops = [(hop, sub) for hop in range(REACH) for sub in range(SUBS)]
    plan = {u: [] for u in range(UNITS + 1)}
    plan[0] += [z_start, functools.partial(kv_level, 1)]
    def send_weights():
        for i in range(3):
            weights[i].wait()
            pairs[i].start()

    forward = [functools.partial(z_forward, 0, sub) for sub in SUB_ORDER]
    plan[0] += [forward[0]]
    plan[1] += [forward[1], send_weights]
    plan[2] += [forward[2], forward[3], functools.partial(kv_level, 2)]
    plan[2] += [functools.partial(start_direct, 1)]
    plan[4] += [functools.partial(kv_level, 3), functools.partial(start_direct, 3)]
    plan[6] += [functools.partial(kv_level, 4), functools.partial(start_direct, 2), wo_start]
    late = {UNITS: 1, UNITS + 2: 2, UNITS + 3: 3, UNITS + 4: 4}

    def unit(u):
        for k in range(UNITS):
            @pl.when(u == k)
            def _(k=k):
                for act in plan[k]:
                    act()
                kvs.wait(k)

        keys = kv[0, pl.ds(2 * u, 2)].reshape(KEYS_UNIT, HD)
        vals = kv[1, pl.ds(2 * u, 2)].reshape(KEYS_UNIT, HD)
        wide = jnp.concatenate([vals, jnp.ones_like(vals)], axis=1)
        for i in range(ROWS // Q_TILE):
            sl = pl.ds(i * Q_TILE, Q_TILE)
            s = lax.dot_general(
                q_n[sl, :], keys, (((1,), (1,)), ((), ())), preferred_element_type=F32
            )
            old = m_ref[sl, :]
            new = jnp.maximum(old, jnp.max(s, axis=1, keepdims=True))
            shrink = jnp.exp2(old - new)
            p = jnp.exp2(s - new[:, :1]).astype(BF16)
            acc_ref[sl, :] = acc_ref[sl, :] * jnp.concatenate([shrink, shrink], axis=1) + jnp.dot(
                p, wide, preferred_element_type=F32
            )
            m_ref[sl, :] = new

    def att_copy(dz, core):
        to = (z + dz) % NZ
        head = pl.ds(pl.multiple_of(z * HD, HD), HD)
        return remote(
            att.at[core * NZ + to], att_all.at[c, :, head], sent.at[9], sent.at[10], z=to, c=core
        )

    def finish_attention():
        for t in range(2 * NZ):
            span = pl.ds(t * TOK, TOK)
            att[t % 2 * NZ + t // 2] = (acc_ref[span, :HD] / acc_ref[span, HD:]).astype(BF16)
        for dz in range(NZ):
            if dz > 0:
                att_copy(dz, c).start()
            att_copy(dz, sib).start()
        att_all[c, :, pl.ds(pl.multiple_of(z * HD, HD), HD)] = att[c * NZ + z]

    piece = HALF // RSUBS

    def rs_copy(way, s, u):
        step = 1 if way == 0 else -1
        return remote(
            rs_buf.at[way, s, u], rs_buf.at[way, s + 1, u],
            ring_sent.at[way], rs_recv.at[way, s, u], z=(z + step) % NZ,
        )

    def ret_copy(p):
        dy, dx = OWNERS[p]
        return remote(
            fin.at[p], ret.at[me], sent.at[3], sent.at[4],
            y=(y + dy) % NY, x=(x + dx) % NX,
        )

    def moe_step(s):
        for k in range(NZ // 2):
            @pl.when(s == k)
            def _(k=k):
                if k == 0:
                    for copy in awaited:
                        copy.wait_recv()
                elif k < REACH:
                    for sub in SUB_ORDER:
                        z_forward(k, sub)
                else:
                    for delta in sorted({k + 1, NZ - k - 1}):
                        wait_direct(DIRECT.index(delta))

        chunk_r = (z - 1 - s + 2 * NZ) % NZ
        chunk_l = (z + 1 + s) % NZ
        act = jnp.concatenate(
            [
                rows[chunk_r, 0 : NE // 2].reshape(HALF, D),
                rows[chunk_l, NE // 2 : NE].reshape(HALF, D),
            ],
            axis=0,
        )
        hidden = []
        for k in range(2):
            gate = jnp.dot(act, wg[k], preferred_element_type=F32)
            up = jnp.dot(act, wu[k], preferred_element_type=F32)
            hidden.append((gate / (1.0 + jnp.exp(-gate)) * up).astype(BF16))
        for k in range(4):
            cols = pl.ds(k * (D // 4), D // 4)
            part[:, cols] = jnp.dot(hidden[0], wd[0, :, cols], preferred_element_type=F32) + jnp.dot(
                hidden[1], wd[1, :, cols], preferred_element_type=F32
            )
        for u in range(RSUBS):
            for way in (0, 1):
                span = pl.ds(way * HALF + u * piece, piece)

                @pl.when(s == 0)
                def _(way=way, u=u, span=span):
                    rs_buf[way, 0, u] = part[span, :].astype(BF16)
                    rs_copy(way, 0, u).start()

                @pl.when(s > 0)
                def _(way=way, u=u, span=span):
                    rs_copy(way, s - 1, u).wait_recv()
                    total = part[span, :] + rs_buf[way, s, u].astype(F32)

                    @pl.when(s < NZ - 1)
                    def _():
                        rs_buf[way, s, u] = total.astype(BF16)
                        rs_copy(way, s, u).start()

                    @pl.when(s == NZ - 1)
                    def _():
                        count = piece // CAP
                        first = way * (NE // 2) + u * count
                        fin[pl.ds(first, count)] = total.astype(BF16).reshape(count, CAP, D)
                        for p in range(first, first + count):
                            if p != SELF:
                                ret_copy(p).start()

    def tick(t, carry):
        @pl.when(t < UNITS)
        def _():
            unit(t)

        @pl.when(t == UNITS - 1)
        def _():
            finish_attention()

        @pl.when((t == EARLY[0]) | (t == EARLY[1]) | ((t >= UNITS) & (t < UNITS + NZ - len(EARLY))))
        def _():
            moe_step(
                jnp.where(t == EARLY[0], 0, jnp.where(t == EARLY[1], 1, t - UNITS + len(EARLY)))
            )

        for at, level in late.items():
            @pl.when(t == at)
            def _(level=level):
                wos.level(level)

        return carry

    lax.fori_loop(0, TICKS, tick, 0)

    own = wo.at[sib, 0]
    remote(own, own, d2d_send.at[3], d2d_recv.at[3], c=sib).wait_recv()
    for pair in range(NE // 2):
        wos.wait(pair)
    heads = att.at[pl.ds(0, 2 * NZ - 1)]
    remote(heads, heads, sent.at[9], sent.at[10], c=sib).wait_recv()
    for slot, (dy, dx) in enumerate(PLACES):
        owner = (y + dy) % NY * NX + (x + dx) % NX
        cols = pl.ds(pl.multiple_of(owner * HD, HD), HD)
        stage[0, :, cols] = (
            jnp.dot(att_all[0], wo[0, slot], preferred_element_type=F32)
            + jnp.dot(att_all[1], wo[1, slot], preferred_element_type=F32)
        ).astype(BF16)
    outs[0].start()
    ret[me] = fin[SELF]
    got = ret.at[pl.ds(0, NE - 1)]
    remote(got, got, sent.at[3], sent.at[4], c=sib).wait_recv()
    back = ret[...].reshape(CH, D)
    dims = (((0,), (0,)), ((), ()))
    stage[1] = (
        lax.dot_general(comb[0], back, dims, preferred_element_type=F32)
        + lax.dot_general(comb[1], back, dims, preferred_element_type=F32)
    ).astype(BF16)
    outs[1].start()

    for span, sem in (
        [(fin.at[pl.ds(0, NE - 1)], sent.at[3]), (rows.at[pl.ds(0, 2 * REACH)], sent.at[2])]
        + [(kv.at[c, pl.ds(1, NE - 1)], sent.at[k]) for k in (0, 1)]
        + [(slots.at[i, pl.ds(0, NE - 1)], a2a_sent.at[i]) for i in range(len(DIRECT))]
        + [(rs_buf.at[way, pl.ds(0, NZ - 1)], ring_sent.at[way]) for way in (0, 1)]
        + [(wo.at[c, pl.ds(1, NE - 1)], sent.at[k]) for k in (5, 6)]
        + [(wo.at[c, 0, pl.ds(0, WO_ROWS - HD)], sent.at[7]), (heads, sent.at[9])]
        + [(wo.at[c, 0], d2d_send.at[3])]
    ):
        remote(span, span, sem, sent.at[4], c=sib).wait_send()
    for copy in pairs:
        copy.wait_send()
    for copy in outs:
        copy.wait()


def fused(*args):
    vmem = pl.BlockSpec(memory_space=pltpu.VMEM)
    hbm = pl.BlockSpec(memory_space=pl.ANY)
    dma = pltpu.SemaphoreType.DMA
    n_direct = len(DIRECT)
    return pl.pallas_call(
        body,
        name="fused_step",
        out_shape=jax.ShapeDtypeStruct((2, TOK, D), BF16),
        in_specs=[hbm] * 3 + [vmem] * 6 + [hbm] * 5,
        out_specs=hbm,
        scratch_shapes=[
            pltpu.VMEM((ROWS, HD), BF16),
            pltpu.VMEM((ROWS, HD), BF16),
            pltpu.VMEM((n_direct, TOK, D), BF16),
            pltpu.VMEM((2, NE, ROWS, HD), BF16),
            pltpu.VMEM((ROWS, HD), BF16),
            pltpu.VMEM((ROWS, HD), F32),
            pltpu.VMEM((ROWS, 2 * HD), F32),
            pltpu.VMEM((2 * NZ, TOK, HD), BF16),
            pltpu.VMEM((n_direct, NE, CAP, D), BF16),
            pltpu.VMEM((NZ, NE, CAP, D), BF16),
            pltpu.VMEM((2, D, FF_DEV), BF16),
            pltpu.VMEM((2, D, FF_DEV), BF16),
            pltpu.VMEM((2, FF_DEV, D), BF16),
            pltpu.VMEM((2, NE, WO_ROWS, HD), BF16),
            pltpu.VMEM((2, TOK, WO_ROWS), BF16),
            pltpu.VMEM((CH, D), F32),
            pltpu.VMEM((2, NZ, RSUBS, HALF // RSUBS, D), BF16),
            pltpu.VMEM((NE, CAP, D), BF16),
            pltpu.VMEM((NE, CAP, D), BF16),
            pltpu.VMEM((CH, TOK), F32),
            pltpu.VMEM((2, CH, TOK), BF16),
            pltpu.VMEM((2, TOK, D), BF16),
            dma((3 + n_direct + 4,)),
            dma((4,)), dma((4,)),
            dma((11,)), dma((n_direct,)), dma((2,)),
            dma((2 * NE - 2,)), dma((UNITS,)), dma((SUBS + n_direct - 1,)), dma((2, REACH, SUBS)),
            dma((2 * NE - 2,)), dma((UNITS,)), dma((2, NZ - 1, RSUBS)), dma((2,)),
        ],
        compiler_params=pltpu.CompilerParams(
            collective_id=0, has_side_effects=True, vmem_limit_bytes=60 * 2**20
        ),
    )(*args)


def on_device(
    queries, keys, values, query_gain, key_gain, out_weight, tokens_b, norm_gain,
    routes, route_weight, gate_weight, up_weight, down_weight,
):
    n_freq = HD // 4
    inverse = np.tile(THETA ** (-np.arange(n_freq) / n_freq), HD // n_freq).astype(np.float32)
    both = fused(
        queries, keys, values, query_gain[None, :], key_gain[None, :], jnp.asarray(inverse)[None, :],
        norm_gain[None, :], routes.T, route_weight.T, tokens_b,
        out_weight, gate_weight[0], up_weight[0], down_weight[0],
    )
    return both[0], both[1]


def solution(mesh):
    torus = Mesh(mesh.devices.reshape(NY, NX, NZ, 2), ("y", "x", "z", "c"))
    ep, tp = ("y", "x"), ("z", "c")
    in_specs = (
        P(ep, tp), P(ep, None), P(ep, None), P(), P(), P(tp, None), P(ep, None), P(),
        P(ep, None), P(ep, None), P(ep, None, tp), P(ep, None, tp), P(ep, tp, None),
    )
    out_specs = (P(ep + tp, None), P(ep + tp, None))
    return jax.shard_map(
        on_device, mesh=torus, in_specs=in_specs, out_specs=out_specs, check_vma=False
    )
```

```python
import functools
import math

import jax
import jax.numpy as jnp
import numpy as np
from jax import lax
from jax.experimental import pallas as pl
from jax.experimental.pallas import tpu as pltpu
from jax.sharding import Mesh
from jax.sharding import PartitionSpec as P

D = 2048
HD = 128
HQ = 16
KVH = 4
FF_DEV = 256
CAP = 8
GRID_W = 64
EPS = 1e-06
THETA = 10000.0

NX = 4
NY = 4
NE = NX * NY
NZ = 8
ROWS = 768
TOK = 48
CH = NE * CAP
HALF = CH // 2

REACH = 2
DIRECT = [0] + list(range(REACH + 1, NZ - REACH))
SUBS = 4
PIECE = NE // SUBS
SUB_ORDER = (1, 3, 0, 2)
RSUBS = 2

OWNERS = [(0, 2), (1, 2), (2, 0), (2, 1), (0, 0), (0, 1), (1, 0), (1, 1)]
OWNERS += [(2, 2), (2, 3), (3, 1), (3, 2), (0, 3), (3, 0), (3, 3), (1, 3)]
SELF = OWNERS.index((0, 0))
OTHERS = [p for p in range(NE) if p != SELF]
NEAR_FIRST = [p for sub in SUB_ORDER for p in range(sub * PIECE, (sub + 1) * PIECE) if p != SELF]

MESH = pl.DeviceIdType.MESH
F32 = jnp.float32
BF16 = jnp.bfloat16

PLACES = [(0, 0)]
PLACES += [(0, 3), (0, 1), (3, 0), (1, 0)]
PLACES += [(3, 3), (3, 1), (1, 3), (1, 1), (0, 2), (2, 0)]
PLACES += [(3, 2), (1, 2), (2, 3), (2, 1)]
PLACES += [(2, 2)]
SLOT = {place: i for i, place in enumerate(PLACES)}
KEYS_UNIT = 2 * ROWS
UNITS = NE * ROWS // KEYS_UNIT
EARLY = (4, 6)
TICKS = UNITS + NZ - len(EARLY)
WO_ROWS = NZ * HD
Q_TILE = 128


def gather_messages():
    out = []
    for half in (0, 1):
        base = half * (ROWS // 2)
        full, quarter = ROWS // 2, ROWS // 4
        prim, sec = ("x", "y") if half == 0 else ("y", "x")

        def slot(p, s, half=half):
            p, s = p % 4, s % 4
            return SLOT[(s, p)] if half == 0 else SLOT[(p, s)]

        def send(level, axis, step, p, s, part, half=half, base=base, full=full, quarter=quarter,
                 prim=prim, sec=sec, slot=slot):
            tp, ts = (p - step, s) if axis == prim else (p, s - step)
            start = base + (quarter if part == 1 else 0)
            rows = full if part is None else quarter
            out.append((level, half, axis, step, slot(p, s), slot(tp, ts), start, rows))

        for axis in (prim, sec):
            for step in (1, -1):
                send(1, axis, step, 0, 0, None)
        for p, step, part in ((-1, 1, 0), (1, -1, 1)):
            send(2, prim, step, p, 0, part)
            send(2, sec, 1, p, 0, None)
            send(2, sec, -1, p, 0, None)
        send(2, sec, 1, 0, -1, 0)
        send(2, sec, -1, 0, 1, 1)
        for p in (-1, 1):
            send(3, sec, 1, p, -1, 0)
            send(3, sec, -1, p, 1, 1)
        send(3, sec, 1, 2, 0, None)
        send(3, sec, -1, 2, 0, None)
        send(4, sec, 1, 2, -1, 0)
        send(4, sec, -1, 2, 1, 1)
    return sorted(out, key=lambda m: m[0])


MESSAGES = gather_messages()
N_MSG = len(MESSAGES)


def body(
    q_hbm, k_hbm, v_hbm, qg_ref, kg_ref, inv_ref, ng_ref, routes_ref, sizes_ref,
    tok_hbm, ow_hbm, wg_hbm, wu_hbm, wd_hbm,
    out_ref,
    q_buf, kv_raw, tok_buf, kv, q_n, m_ref, acc_ref, att, slots, rows,
    wg, wu, wd, wo, att_all, part, rs_buf, fin, ret, mat_ref, comb, stage,
    in_sem, d2d_send, d2d_recv, sent, a2a_sent, ring_sent, kv_recv, kvd_recv, a2a_recv, z_recv,
    wo_recv, wod_recv, rs_recv, out_sem,
):
    y = lax.axis_index("y")
    x = lax.axis_index("x")
    z = lax.axis_index("z")
    c = lax.axis_index("c")
    me = y * NX + x
    sib = 1 - c

    def remote(src, dst, send_sem, recv_sem, **device):
        return pltpu.make_async_remote_copy(
            src_ref=src, dst_ref=dst, send_sem=send_sem, recv_sem=recv_sem,
            device_id=device, device_id_type=MESH,
        )

    barrier = pltpu.get_barrier_semaphore()
    partners = [{"y": (y + dy) % NY, "x": (x + dx) % NX} for dy, dx in PLACES[1:]]
    partners += [{"z": (z + dz) % NZ} for dz in range(1, NZ)]
    partners += [{"z": (z + dz) % NZ, "c": sib} for dz in range(NZ)]
    for partner in partners:
        pl.semaphore_signal(barrier, inc=1, device_id=partner, device_id_type=MESH)

    outs = [pltpu.make_async_copy(stage.at[i], out_ref.at[i], out_sem.at[i]) for i in range(2)]

    head = (2 * z + c) // 4
    lane = pl.ds(pl.multiple_of(head * HD, HD), HD)
    loads = [
        pltpu.make_async_copy(k_hbm.at[:, lane], kv_raw, in_sem.at[0]),
        pltpu.make_async_copy(v_hbm.at[:, lane], kv.at[1, 0], in_sem.at[1]),
        pltpu.make_async_copy(q_hbm, q_buf, in_sem.at[2]),
    ]
    for i, delta in enumerate(DIRECT):
        blk = (z + delta) % NZ * 2 + c
        loads.append(
            pltpu.make_async_copy(
                tok_hbm.at[pl.ds(pl.multiple_of(blk * TOK, TOK), TOK), :],
                tok_buf.at[i], in_sem.at[3 + i],
            )
        )
    for copy in loads:
        copy.start()
    weights = []
    for i, (src, dst) in enumerate(((wg_hbm, wg), (wu_hbm, wu), (wd_hbm, wd))):
        weights.append(pltpu.make_async_copy(src, dst.at[c], in_sem.at[3 + len(DIRECT) + i]))
    slab = pl.ds(pl.multiple_of(me * HD, HD), HD)
    wo_own = wo.at[c, 0, pl.ds(pl.multiple_of(z * HD, HD), HD)]
    wo_load = pltpu.make_async_copy(ow_hbm.at[:, slab], wo_own, in_sem.at[6 + len(DIRECT)])
    wo_load.start()
    for copy in weights:
        copy.start()

    def block_of(ref, blk):
        return pltpu.roll(ref[...], (ROWS - blk * TOK) % ROWS, 1)[:, :TOK]

    def make_slots(i):
        delta = DIRECT[i]
        blk = (z + delta) % NZ * 2 + c
        loads[3 + i].wait()
        field = tok_buf[i].astype(F32)
        scale = lax.rsqrt(jnp.mean(field * field, axis=1, keepdims=True) + EPS)
        normed = (field * scale * ng_ref[...]).astype(BF16)
        j = lax.broadcasted_iota(jnp.int32, (CH, TOK), 0)
        expert, rank = j // CAP, j % CAP
        picks = block_of(routes_ref, blk)
        r0, r1 = picks[0:1], picks[1:2]
        hot = ((r0 == expert) | (r1 == expert)).astype(F32)
        before = (
            lax.broadcasted_iota(jnp.int32, (TOK, TOK), 0)
            < lax.broadcasted_iota(jnp.int32, (TOK, TOK), 1)
        ).astype(BF16)
        count = jnp.dot(hot.astype(BF16), before, preferred_element_type=F32)
        mat = jnp.where(count == rank.astype(F32), hot, 0.0)
        if i == 0:
            mat_ref[...] = mat
        slots[i] = jnp.dot(mat.astype(BF16), normed, preferred_element_type=F32).astype(
            BF16
        ).reshape(NE, CAP, D)

    def a2a(i, p):
        dy, dx = OWNERS[p]
        ty, tx = (y - dy + NY) % NY, (x - dx + NX) % NX
        return remote(
            slots.at[i, ty * NX + tx], rows.at[(z + DIRECT[i]) % NZ, p],
            a2a_sent.at[i], a2a_recv.at[p // PIECE if i == 0 else SUBS + i - 1], y=ty, x=tx,
        )

    def start_direct(i):
        for p in NEAR_FIRST:
            a2a(i, p).start()
        rows[(z + DIRECT[i]) % NZ, SELF] = slots[i, me]

    def wait_rows(i, sem, first, count):
        span = rows.at[(z + DIRECT[i]) % NZ, pl.ds(first, count)]
        remote(span, span, a2a_sent.at[i], a2a_recv.at[sem], c=sib).wait_recv()

    def wait_own(sub):
        wait_rows(0, sub, sub * PIECE, PIECE - (SELF // PIECE == sub))

    def wait_direct(i):
        wait_rows(i, SUBS + i - 1, 0, NE - 1)

    make_slots(0)
    pl.semaphore_wait(barrier, len(partners))
    start_direct(0)

    own = 2 * z + c
    j = lax.broadcasted_iota(jnp.int32, (CH, TOK), 0)
    picks = block_of(routes_ref, own)
    sizes = block_of(sizes_ref, own)
    w0, w1 = sizes[0:1], sizes[1:2]
    share = jnp.where(picks[0:1] == j // CAP, w0, w1) / (w0 + w1)
    combine = jnp.where(mat_ref[...] > 0.5, share, 0.0)
    high = combine.astype(BF16)
    comb[0] = high
    comb[1] = (combine - high.astype(F32)).astype(BF16)

    lane_of = lax.broadcasted_iota(jnp.int32, (GRID_W, HD), 1)
    pi = lax.broadcasted_iota(jnp.int32, (HD, HD), 0)
    pj = lax.broadcasted_iota(jnp.int32, (HD, HD), 1)
    first_half = pj % 64 < 32
    swap = jnp.where(
        first_half & (pi == pj + 32), -1.0, jnp.where(~first_half & (pi == pj - 32), 1.0, 0.0)
    ).astype(BF16)

    row_pos = me * (ROWS // GRID_W) + lax.broadcasted_iota(jnp.int32, (16, HD), 0)
    col_pos = lax.broadcasted_iota(jnp.int32, (GRID_W, HD), 0)
    by_row = row_pos.astype(F32) * inv_ref[...]
    by_col = col_pos.astype(F32) * inv_ref[...]
    cos_row, sin_row = jnp.cos(by_row), jnp.sin(by_row)
    cos_col, sin_col = jnp.cos(by_col), jnp.sin(by_col)

    def turn(src, gain_ref, factor, store):
        gain = gain_ref[...]
        other = jnp.where(
            lax.broadcasted_iota(jnp.int32, (1, HD), 1) % 64 < 32,
            pltpu.roll(gain, HD - 32, 1), pltpu.roll(gain, 32, 1),
        )
        for g in range(ROWS // GRID_W):
            raw = src[g * GRID_W : (g + 1) * GRID_W, :]
            val = raw.astype(F32)
            inv = lax.rsqrt(jnp.mean(val * val, axis=1, keepdims=True) + EPS)
            if factor != 1.0:
                inv = inv * factor
            turned = jnp.dot(raw, swap, preferred_element_type=F32)
            cosine = jnp.where(lane_of < 64, cos_row[g : g + 1, :], cos_col)
            sine = jnp.where(lane_of < 64, sin_row[g : g + 1, :], sin_col)
            store(g, ((val * (gain * cosine) + turned * (other * sine)) * inv).astype(BF16))

    def store_key(g, val):
        kv[0, 0, g * GRID_W : (g + 1) * GRID_W, :] = val

    def store_query(g, val):
        q_n[g * GRID_W : (g + 1) * GRID_W, :] = val

    loads[0].wait()
    turn(kv_raw, kg_ref, 1.0, store_key)
    loads[1].wait()

    class Gather:
        def __init__(self, buf, size, first, arrived, crossed):
            self.buf, self.size, self.arrived, self.crossed = buf, size, arrived, crossed
            self.ring, self.across_sem = sent.at[first], sent.at[first + 1]

        def copy(self, n):
            _, half, axis, step, src, dst, start, count = MESSAGES[n]
            here = y if axis == "y" else x
            span = pl.ds(start * self.size // ROWS, count * self.size // ROWS)
            return remote(
                self.buf.at[c, src, span], self.buf.at[c, dst, span], self.ring,
                self.arrived.at[(dst - 1) * 2 + half], **{axis: (here + step) % 4},
            )

        def start(self):
            for n, msg in enumerate(MESSAGES):
                if msg[0] == 1:
                    self.copy(n).start()

        def level(self, level):
            for dst, half in dict.fromkeys((m[5], m[1]) for m in MESSAGES if m[0] == level):
                span = self.buf.at[c, dst, pl.ds(half * (self.size // 2), self.size // 2)]
                remote(span, span, self.ring, self.arrived.at[(dst - 1) * 2 + half], c=sib).wait_recv()
                for k, later in enumerate(MESSAGES):
                    if later[0] == level + 1 and later[1] == half and later[4] == dst:
                        self.copy(k).start()
                remote(span, span, self.across_sem, self.crossed.at[dst // 2], c=sib).start()

        def wait(self, pair):
            first = max(2 * pair, 1)
            span = self.buf.at[sib, pl.ds(first, 2 * pair + 2 - first)]
            remote(span, span, self.across_sem, self.crossed.at[pair], c=sib).wait_recv()

    kvs = Gather(kv, ROWS, 0, kv_recv, kvd_recv)
    wos = Gather(wo, WO_ROWS, 5, wo_recv, wod_recv)
    kv_level = kvs.level

    def wo_copy(dz):
        return remote(wo_own, wo_own, sent.at[7], sent.at[8], z=(z + dz) % NZ)

    wo_load.wait()
    for dz in range(1, NZ):
        wo_copy(dz).start()

    def wo_start():
        span = wo.at[c, 0, pl.ds(0, WO_ROWS - HD)]
        remote(span, span, sent.at[7], sent.at[8], c=sib).wait_recv()
        own = wo.at[c, 0]
        remote(own, own, d2d_send.at[3], d2d_recv.at[3], c=sib).start()
        wos.start()

    loads[2].wait()
    turn(q_buf, qg_ref, HD ** (-0.5) * math.log2(math.e), store_query)

    pairs = [
        remote(buf.at[c], buf.at[c], d2d_send.at[i], d2d_recv.at[i], c=sib)
        for i, buf in enumerate((wg, wu, wd))
    ]
    awaited = [
        remote(buf.at[sib], buf.at[sib], d2d_send.at[i], d2d_recv.at[i], c=sib)
        for i, buf in enumerate((wg, wu, wd))
    ]

    for i in range(1, len(DIRECT)):
        make_slots(i)

    def z_copy(way, hop, sub):
        step = 1 if way == 0 else -1
        chunk = (z - step * hop) % NZ
        span = pl.ds(sub * PIECE, PIECE)
        return remote(
            rows.at[chunk, span], rows.at[chunk, span],
            sent.at[2], z_recv.at[way, hop, sub], z=(z + step) % NZ,
        )

    def z_wait(way, hop, sub):
        step = 1 if way == 0 else -1
        chunk = (z - step * (hop + 1)) % NZ
        span = pl.ds(sub * PIECE, PIECE)
        return remote(
            rows.at[chunk, span], rows.at[chunk, span],
            sent.at[2], z_recv.at[way, hop, sub], z=(z + step) % NZ,
        )

    def z_start():
        for sub in SUB_ORDER:
            wait_own(sub)
            if sub == SUB_ORDER[1]:
                kvs.start()
            for way in (0, 1):
                z_copy(way, 0, sub).start()

    def z_forward(hop, sub):
        for way in (0, 1):
            z_wait(way, hop, sub).wait_recv()
            if hop + 1 < REACH:
                z_copy(way, hop + 1, sub).start()

    m_ref[...] = jnp.full_like(m_ref, -1e30)
    acc_ref[...] = jnp.zeros_like(acc_ref)

    hops = [(hop, sub) for hop in range(REACH) for sub in range(SUBS)]
    plan = {u: [] for u in range(UNITS + 1)}
    plan[0] += [z_start, functools.partial(kv_level, 1)]
    def send_weights():
        for i in range(3):
            weights[i].wait()
            pairs[i].start()

    forward = [functools.partial(z_forward, 0, sub) for sub in SUB_ORDER]
    plan[0] += [forward[0]]
    plan[1] += [forward[1], send_weights]
    plan[2] += [forward[2], forward[3], functools.partial(kv_level, 2)]
    plan[2] += [functools.partial(start_direct, 1)]
    plan[4] += [functools.partial(kv_level, 3), functools.partial(start_direct, 3)]
    plan[6] += [functools.partial(kv_level, 4), functools.partial(start_direct, 2), wo_start]
    late = {UNITS: 1, UNITS + 2: 2, UNITS + 3: 3}

    def unit(u):
        for k in range(UNITS):
            @pl.when(u == k)
            def _(k=k):
                for act in plan[k]:
                    act()
                kvs.wait(k)

        keys = kv[0, pl.ds(2 * u, 2)].reshape(KEYS_UNIT, HD)
        vals = kv[1, pl.ds(2 * u, 2)].reshape(KEYS_UNIT, HD)
        wide = jnp.concatenate([vals, jnp.ones_like(vals)], axis=1)
        for i in range(ROWS // Q_TILE):
            sl = pl.ds(i * Q_TILE, Q_TILE)
            s = lax.dot_general(
                q_n[sl, :], keys, (((1,), (1,)), ((), ())), preferred_element_type=F32
            )
            old = m_ref[sl, :]
            new = jnp.maximum(old, jnp.max(s, axis=1, keepdims=True))
            shrink = jnp.exp2(old - new)
            p = jnp.exp2(s - new[:, :1]).astype(BF16)
            acc_ref[sl, :] = acc_ref[sl, :] * jnp.concatenate([shrink, shrink], axis=1) + jnp.dot(
                p, wide, preferred_element_type=F32
            )
            m_ref[sl, :] = new

    def att_copy(dz, core):
        to = (z + dz) % NZ
        head = pl.ds(pl.multiple_of(z * HD, HD), HD)
        return remote(
            att.at[core * NZ + to], att_all.at[c, :, head], sent.at[9], sent.at[10], z=to, c=core
        )

    def finish_attention():
        for t in range(2 * NZ):
            span = pl.ds(t * TOK, TOK)
            att[t % 2 * NZ + t // 2] = (acc_ref[span, :HD] / acc_ref[span, HD:]).astype(BF16)
        for dz in range(NZ):
            if dz > 0:
                att_copy(dz, c).start()
            att_copy(dz, sib).start()
        att_all[c, :, pl.ds(pl.multiple_of(z * HD, HD), HD)] = att[c * NZ + z]

    piece = HALF // RSUBS

    def rs_copy(way, s, u):
        step = 1 if way == 0 else -1
        return remote(
            rs_buf.at[way, s, u], rs_buf.at[way, s + 1, u],
            ring_sent.at[way], rs_recv.at[way, s, u], z=(z + step) % NZ,
        )

    def ret_copy(p):
        dy, dx = OWNERS[p]
        return remote(
            fin.at[p], ret.at[me], sent.at[3], sent.at[4],
            y=(y + dy) % NY, x=(x + dx) % NX,
        )

    def moe_step(s):
        for k in range(NZ // 2):
            @pl.when(s == k)
            def _(k=k):
                if k == 0:
                    for copy in awaited:
                        copy.wait_recv()
                elif k < REACH:
                    for sub in SUB_ORDER:
                        z_forward(k, sub)
                else:
                    for delta in sorted({k + 1, NZ - k - 1}):
                        wait_direct(DIRECT.index(delta))

        chunk_r = (z - 1 - s + 2 * NZ) % NZ
        chunk_l = (z + 1 + s) % NZ
        act = jnp.concatenate(
            [
                rows[chunk_r, 0 : NE // 2].reshape(HALF, D),
                rows[chunk_l, NE // 2 : NE].reshape(HALF, D),
            ],
            axis=0,
        )
        hidden = []
        for k in range(2):
            gate = jnp.dot(act, wg[k], preferred_element_type=F32)
            up = jnp.dot(act, wu[k], preferred_element_type=F32)
            hidden.append((gate / (1.0 + jnp.exp(-gate)) * up).astype(BF16))
        for k in range(4):
            cols = pl.ds(k * (D // 4), D // 4)
            part[:, cols] = jnp.dot(hidden[0], wd[0, :, cols], preferred_element_type=F32) + jnp.dot(
                hidden[1], wd[1, :, cols], preferred_element_type=F32
            )
        for u in range(RSUBS):
            for way in (0, 1):
                span = pl.ds(way * HALF + u * piece, piece)

                @pl.when(s == 0)
                def _(way=way, u=u, span=span):
                    rs_buf[way, 0, u] = part[span, :].astype(BF16)
                    rs_copy(way, 0, u).start()

                @pl.when(s > 0)
                def _(way=way, u=u, span=span):
                    rs_copy(way, s - 1, u).wait_recv()
                    total = part[span, :] + rs_buf[way, s, u].astype(F32)

                    @pl.when(s < NZ - 1)
                    def _():
                        rs_buf[way, s, u] = total.astype(BF16)
                        rs_copy(way, s, u).start()

                    @pl.when(s == NZ - 1)
                    def _():
                        count = piece // CAP
                        first = way * (NE // 2) + u * count
                        fin[pl.ds(first, count)] = total.astype(BF16).reshape(count, CAP, D)
                        for p in range(first, first + count):
                            if p != SELF:
                                ret_copy(p).start()

    def tick(t, carry):
        @pl.when(t < UNITS)
        def _():
            unit(t)

        @pl.when(t == UNITS - 1)
        def _():
            finish_attention()

        @pl.when((t == EARLY[0]) | (t == EARLY[1]) | ((t >= UNITS) & (t < UNITS + NZ - len(EARLY))))
        def _():
            moe_step(
                jnp.where(t == EARLY[0], 0, jnp.where(t == EARLY[1], 1, t - UNITS + len(EARLY)))
            )

        for at, level in late.items():
            @pl.when(t == at)
            def _(level=level):
                wos.level(level)

        return carry

    lax.fori_loop(0, TICKS, tick, 0)

    own = wo.at[sib, 0]
    remote(own, own, d2d_send.at[3], d2d_recv.at[3], c=sib).wait_recv()
    wos.level(4)
    for pair in range(NE // 2):
        wos.wait(pair)
    heads = att.at[pl.ds(0, 2 * NZ - 1)]
    remote(heads, heads, sent.at[9], sent.at[10], c=sib).wait_recv()
    for slot, (dy, dx) in enumerate(PLACES):
        owner = (y + dy) % NY * NX + (x + dx) % NX
        cols = pl.ds(pl.multiple_of(owner * HD, HD), HD)
        stage[0, :, cols] = (
            jnp.dot(att_all[0], wo[0, slot], preferred_element_type=F32)
            + jnp.dot(att_all[1], wo[1, slot], preferred_element_type=F32)
        ).astype(BF16)
    outs[0].start()
    ret[me] = fin[SELF]
    got = ret.at[pl.ds(0, NE - 1)]
    remote(got, got, sent.at[3], sent.at[4], c=sib).wait_recv()
    back = ret[...].reshape(CH, D)
    dims = (((0,), (0,)), ((), ()))
    stage[1] = (
        lax.dot_general(comb[0], back, dims, preferred_element_type=F32)
        + lax.dot_general(comb[1], back, dims, preferred_element_type=F32)
    ).astype(BF16)
    outs[1].start()

    for span, sem in (
        [(fin.at[pl.ds(0, NE - 1)], sent.at[3]), (rows.at[pl.ds(0, 2 * REACH)], sent.at[2])]
        + [(kv.at[c, pl.ds(1, NE - 1)], sent.at[k]) for k in (0, 1)]
        + [(slots.at[i, pl.ds(0, NE - 1)], a2a_sent.at[i]) for i in range(len(DIRECT))]
        + [(rs_buf.at[way, pl.ds(0, NZ - 1)], ring_sent.at[way]) for way in (0, 1)]
        + [(wo.at[c, pl.ds(1, NE - 1)], sent.at[k]) for k in (5, 6)]
        + [(wo.at[c, 0, pl.ds(0, WO_ROWS - HD)], sent.at[7]), (heads, sent.at[9])]
        + [(wo.at[c, 0], d2d_send.at[3])]
    ):
        remote(span, span, sem, sent.at[4], c=sib).wait_send()
    for copy in pairs:
        copy.wait_send()
    for copy in outs:
        copy.wait()


def fused(*args):
    vmem = pl.BlockSpec(memory_space=pltpu.VMEM)
    hbm = pl.BlockSpec(memory_space=pl.ANY)
    dma = pltpu.SemaphoreType.DMA
    n_direct = len(DIRECT)
    return pl.pallas_call(
        body,
        name="fused_step",
        out_shape=jax.ShapeDtypeStruct((2, TOK, D), BF16),
        in_specs=[hbm] * 3 + [vmem] * 6 + [hbm] * 5,
        out_specs=hbm,
        scratch_shapes=[
            pltpu.VMEM((ROWS, HD), BF16),
            pltpu.VMEM((ROWS, HD), BF16),
            pltpu.VMEM((n_direct, TOK, D), BF16),
            pltpu.VMEM((2, NE, ROWS, HD), BF16),
            pltpu.VMEM((ROWS, HD), BF16),
            pltpu.VMEM((ROWS, HD), F32),
            pltpu.VMEM((ROWS, 2 * HD), F32),
            pltpu.VMEM((2 * NZ, TOK, HD), BF16),
            pltpu.VMEM((n_direct, NE, CAP, D), BF16),
            pltpu.VMEM((NZ, NE, CAP, D), BF16),
            pltpu.VMEM((2, D, FF_DEV), BF16),
            pltpu.VMEM((2, D, FF_DEV), BF16),
            pltpu.VMEM((2, FF_DEV, D), BF16),
            pltpu.VMEM((2, NE, WO_ROWS, HD), BF16),
            pltpu.VMEM((2, TOK, WO_ROWS), BF16),
            pltpu.VMEM((CH, D), F32),
            pltpu.VMEM((2, NZ, RSUBS, HALF // RSUBS, D), BF16),
            pltpu.VMEM((NE, CAP, D), BF16),
            pltpu.VMEM((NE, CAP, D), BF16),
            pltpu.VMEM((CH, TOK), F32),
            pltpu.VMEM((2, CH, TOK), BF16),
            pltpu.VMEM((2, TOK, D), BF16),
            dma((3 + n_direct + 4,)),
            dma((4,)), dma((4,)),
            dma((11,)), dma((n_direct,)), dma((2,)),
            dma((2 * NE - 2,)), dma((UNITS,)), dma((SUBS + n_direct - 1,)), dma((2, REACH, SUBS)),
            dma((2 * NE - 2,)), dma((UNITS,)), dma((2, NZ - 1, RSUBS)), dma((2,)),
        ],
        compiler_params=pltpu.CompilerParams(
            collective_id=0, has_side_effects=True, vmem_limit_bytes=60 * 2**20
        ),
    )(*args)


def on_device(
    queries, keys, values, query_gain, key_gain, out_weight, tokens_b, norm_gain,
    routes, route_weight, gate_weight, up_weight, down_weight,
):
    n_freq = HD // 4
    inverse = np.tile(THETA ** (-np.arange(n_freq) / n_freq), HD // n_freq).astype(np.float32)
    both = fused(
        queries, keys, values, query_gain[None, :], key_gain[None, :], jnp.asarray(inverse)[None, :],
        norm_gain[None, :], routes.T, route_weight.T, tokens_b,
        out_weight, gate_weight[0], up_weight[0], down_weight[0],
    )
    return both[0], both[1]


def solution(mesh):
    torus = Mesh(mesh.devices.reshape(NY, NX, NZ, 2), ("y", "x", "z", "c"))
    ep, tp = ("y", "x"), ("z", "c")
    in_specs = (
        P(ep, tp), P(ep, None), P(ep, None), P(), P(), P(tp, None), P(ep, None), P(),
        P(ep, None), P(ep, None), P(ep, None, tp), P(ep, None, tp), P(ep, tp, None),
    )
    out_specs = (P(ep + tp, None), P(ep + tp, None))
    return jax.shard_map(
        on_device, mesh=torus, in_specs=in_specs, out_specs=out_specs, check_vma=False
    )
```
